32 devices in a mesh: sp: 8 (over z, y), tp: 4 (over x, core).
Axes of the slice: x: 2, y: 2, z: 4, core: 2. Of those that a mesh axis runs over, the one named last changes fastest.
Arguments:
- resid_in: bfloat16 [1024, 2048], P('sp'), may hold values from -6 to 6
- query_plain: bfloat16 [1024, 2048], P('sp', 'tp'), may hold values from -480 to 480, as said below
- query_turn: bfloat16 [1024, 1024], P('sp', 'tp'), may hold values from -16 to 16
- latent_raw: bfloat16 [1024, 256], P('sp'), may hold values from -6 to 6
- shared_key: bfloat16 [1024, 32], P('sp'), may hold values from -6 to 6
- latent_gain: float32 [256], replicated, may hold values from 0.1 to 1.9
- key_up: bfloat16 [256, 2048], P(None, 'tp'), may hold values from -0.375 to 0.375
- value_up: bfloat16 [256, 2048], P(None, 'tp'), may hold values from -0.375 to 0.375
- out_weight: bfloat16 [2048, 2048], P('tp'), may hold values from -0.5 to 0.5
- mixer_gain: float32 [2048], replicated, may hold values from 0.1 to 1.9
- gate_weight: bfloat16 [2048, 5632], P('sp', 'tp'), may hold values from -0.125 to 0.125
- up_weight: bfloat16 [2048, 5632], P('sp', 'tp'), may hold values from -0.125 to 0.125
- down_weight: bfloat16 [5632, 2048], P('tp', 'sp'), may hold values from -0.15625 to 0.15625
Outputs:
- layer_out: bfloat16 [1024, 2048], P(('sp', 'tp'))
The draws below stay inside these ranges and needn't reach their ends.
Inputs may be any that keep to these rules, and one draw needn't show every extreme that they name: Entries of query_plain lie in this range.
All inputs are finite; a program needn't handle non-finite values.
Results may differ from the reference program's by a relative error of at most 0.014.
The reference program's roundings to bfloat16 on the way (of `query_rot`, `key_rot`, `latent`, `weight`, `attended`, `normed` and `hidden`) count: a program that leaves them out, or rounds other values in their place, can miss the bound.
Values may be sent and summed in bfloat16 or wider, within the bound.
A program may use at most 128 MiB of HBM per device.

```python
import math
import jax
import jax.numpy as jnp
from jax import lax

D = 2048
H = 32
NOPE = 64
ROPE = 32
V = 64
KV = 256
FF = 5632
HV = 2048
TOKENS = 1024


def draw_query_plain(key, part):
    first = jax.random.fold_in(jax.random.fold_in(key, 11), 0)
    base = jnp.clip(jax.random.normal(first, (TOKENS, H * NOPE), jnp.float32), -6.0, 6.0) * 2.5
    return base.astype(jnp.bfloat16)


def level_of(key, shape, cuts, least, top_value):
    def one(dim, parts):
        heights = jax.random.uniform(jax.random.fold_in(jax.random.fold_in(key, 6), dim), (parts,), jnp.float32, least / len(cuts), top_value / len(cuts))
        return jnp.repeat(jnp.exp(heights), shape[dim] // parts).reshape((-1,) + (1,) * (len(shape) - dim - 1))

    factor_of = one(*cuts[0])
    for cut in cuts[1:]:
        factor_of = factor_of * one(*cut)
    return factor_of


def scatter_about(key, dims, spread, limit, cuts=(), held_as=jnp.bfloat16):
    result = spread * jax.random.normal(key, dims, jnp.float32)
    if cuts:
        result = result * level_of(key, dims, cuts, -0.22, 0.18)
    return jnp.clip(result, -limit, limit).astype(held_as)


def setup_inputs(seed: int = 0) -> dict:
    keys = jax.random.split(jax.random.key(seed), 14)
    resid_in = scatter_about(keys[0], (TOKENS, D), 1.0, 6.0, ((0, 8),))
    query_plain = draw_query_plain(jax.random.fold_in(keys[13], 71), 0)
    query_turn = scatter_about(keys[2], (TOKENS, H * ROPE), 2.5, 16.0, ((0, 8), (1, 4)))
    latent_raw = scatter_about(keys[3], (TOKENS, KV), 1.0, 6.0, ((0, 8),))
    shared_key = scatter_about(keys[4], (TOKENS, ROPE), 1.0, 6.0, ((0, 8),))
    latent_gain = jnp.clip(1.0 + 0.18 * jax.random.normal(keys[5], (KV,), jnp.float32), 0.1, 1.9)
    key_up = scatter_about(keys[6], (KV, H * NOPE), KV ** -0.5, 0.375, ((1, 4),))
    value_up = scatter_about(keys[7], (KV, HV), KV ** -0.5, 0.375, ((1, 4),))
    out_weight = scatter_about(keys[8], (HV, D), (HV // 16) ** -0.5, 0.5, ((0, 4),))
    mixer_gain = jnp.clip(1.0 + 0.18 * jax.random.normal(keys[9], (D,), jnp.float32), 0.1, 1.9)
    gate_weight = scatter_about(keys[10], (D, FF), D ** -0.5, 0.125, ((0, 8), (1, 4)))
    up_weight = scatter_about(keys[11], (D, FF), D ** -0.5, 0.125, ((0, 8), (1, 4)))
    down_weight = scatter_about(keys[12], (FF, D), (FF // 4) ** -0.5, 0.15625, ((0, 4), (1, 8)))
    return dict(resid_in=resid_in, query_plain=query_plain, query_turn=query_turn, latent_raw=latent_raw, shared_key=shared_key, latent_gain=latent_gain, key_up=key_up, value_up=value_up, out_weight=out_weight, mixer_gain=mixer_gain, gate_weight=gate_weight, up_weight=up_weight, down_weight=down_weight)


def rotate(values, cosine, sine):
    half_width = values.shape[-1] // 2
    first = values[..., :half_width]
    second = values[..., half_width:]
    return jnp.concatenate([first * cosine - second * sine, first * sine + second * cosine], axis=-1)

def rms_scale(values, gain):
    return values * lax.rsqrt(lax.optimization_barrier(jnp.mean(values * values, axis=-1, keepdims=True)) + 1e-06) * gain.astype(jnp.float32)

def reference(resid_in, query_plain, query_turn, latent_raw, shared_key, latent_gain, key_up, value_up, out_weight, mixer_gain, gate_weight, up_weight, down_weight):
    position = jnp.arange(TOKENS, dtype=jnp.int32).astype(jnp.float32)
    inverse = 10000.0 ** (-jnp.arange(0, ROPE, 2, dtype=jnp.float32) / ROPE)
    angles = position[:, None] * inverse[None, :]
    cosine = jnp.cos(angles)
    sine = jnp.sin(angles)
    query_rot = rotate(query_turn.astype(jnp.float32).reshape(TOKENS, H, ROPE), cosine[:, None, :], sine[:, None, :]).astype(jnp.bfloat16)
    key_rot = rotate(shared_key.astype(jnp.float32), cosine, sine).astype(jnp.bfloat16)
    latent = rms_scale(latent_raw.astype(jnp.float32), latent_gain).astype(jnp.bfloat16)
    key_plain = jnp.dot(latent, key_up, preferred_element_type=jnp.float32).astype(jnp.bfloat16).reshape(TOKENS, H, NOPE)
    values = jnp.dot(latent, value_up, preferred_element_type=jnp.float32).astype(jnp.bfloat16).reshape(TOKENS, H, V)
    query_heads = query_plain.reshape(TOKENS, H, NOPE)
    block_len = math.gcd(TOKENS, 128)
    block_count = TOKENS // block_len
    scale = (NOPE + ROPE) ** (-0.5)
    key_plain32 = key_plain.astype(jnp.float32)
    key_rot32 = key_rot.astype(jnp.float32)
    values32 = values.astype(jnp.float32)

    def attend(blocks):
        query_block, rot_block = blocks
        score = jnp.einsum('qhd,khd->hqk', query_block.astype(jnp.float32), key_plain32)
        score = score + jnp.einsum('qhr,kr->hqk', rot_block.astype(jnp.float32), key_rot32)
        score = score * scale
        top = lax.optimization_barrier(jnp.max(score, axis=-1, keepdims=True))
        expo = jnp.exp(score - top)
        total = lax.optimization_barrier(jnp.sum(expo, axis=-1))
        weight = expo.astype(jnp.bfloat16).astype(jnp.float32)
        summed = jnp.einsum('hqk,khd->qhd', weight, values32)
        return (summed / total.T[:, :, None]).astype(jnp.bfloat16)
    attended = lax.map(attend, (query_heads.reshape(block_count, block_len, H, NOPE), query_rot.reshape(block_count, block_len, H, ROPE)))
    attended = attended.reshape(TOKENS, H * V)
    mid = resid_in.astype(jnp.float32) + jnp.dot(attended, out_weight, preferred_element_type=jnp.float32)
    normed = rms_scale(mid, mixer_gain).astype(jnp.bfloat16)
    gate_sum = jnp.dot(normed, gate_weight, preferred_element_type=jnp.float32)
    up_sum = jnp.dot(normed, up_weight, preferred_element_type=jnp.float32)
    hidden = (jax.nn.silu(gate_sum) * up_sum).astype(jnp.bfloat16)
    down_sum = jnp.dot(hidden, down_weight, preferred_element_type=jnp.float32)
    return (mid + 0.5 * down_sum).astype(jnp.bfloat16)
```

```python
import functools
import math

import jax
import jax.numpy as jnp
from jax import lax
from jax.experimental import pallas as pl
from jax.experimental.pallas import tpu as pltpu
from jax.sharding import PartitionSpec as P

NOPE = 64
ROPE = 32
V = 64


def rotate(values, cosine, sine):
    half_width = values.shape[-1] // 2
    first = values[..., :half_width]
    second = values[..., half_width:]
    return jnp.concatenate(
        [first * cosine - second * sine, first * sine + second * cosine], axis=-1
    )


def rms_scale(values, gain):
    return values * lax.rsqrt(jnp.mean(values * values, axis=-1, keepdims=True) + 1e-06) * gain


def plain_layer(
    resid_in,
    query_plain,
    query_turn,
    latent_raw,
    shared_key,
    latent_gain,
    key_up,
    value_up,
    out_weight,
    mixer_gain,
    gate_weight,
    up_weight,
    down_weight,
):
    tok_rows = resid_in.shape[0]
    head_count = query_plain.shape[1] // NOPE
    part_rows = tok_rows // lax.axis_size("tp")
    offset = lax.axis_index("sp") * tok_rows
    position = (offset + jnp.arange(tok_rows, dtype=jnp.int32)).astype(jnp.float32)
    inverse = 10000.0 ** (-jnp.arange(0, ROPE, 2, dtype=jnp.float32) / ROPE)
    angles = position[:, None] * inverse[None, :]
    cosine = jnp.cos(angles)
    sine = jnp.sin(angles)
    query_heads = query_plain.reshape(tok_rows, head_count, NOPE)
    query_rot = rotate(
        query_turn.reshape(tok_rows, head_count, ROPE).astype(jnp.float32),
        cosine[:, None, :],
        sine[:, None, :],
    ).astype(jnp.bfloat16)
    latent = rms_scale(latent_raw.astype(jnp.float32), latent_gain).astype(jnp.bfloat16)
    key_rot = rotate(shared_key.astype(jnp.float32), cosine, sine).astype(jnp.bfloat16)
    softmax_scale = (NOPE + ROPE) ** (-0.5)

    def attend_block(state, key_plain, values, key_pos):
        run_max, run_total, run_acc = state
        score = jnp.einsum(
            "qhd,khd->hqk", query_heads, key_plain, preferred_element_type=jnp.float32
        )
        score = score + jnp.einsum(
            "qhr,kr->hqk", query_rot, key_pos, preferred_element_type=jnp.float32
        )
        score = score * softmax_scale
        new_max = jnp.maximum(run_max, jnp.max(score, axis=-1))
        shrink = jnp.exp(run_max - new_max)
        expo = jnp.exp(score - new_max[:, :, None])
        run_total = run_total * shrink + jnp.sum(expo, axis=-1)
        run_acc = run_acc * shrink.T[:, :, None] + jnp.einsum(
            "hqk,khd->qhd", expo.astype(jnp.bfloat16), values, preferred_element_type=jnp.float32
        )
        return (new_max, run_total, run_acc)

    start_state = (
        jnp.full((head_count, tok_rows), -jnp.inf, jnp.float32),
        jnp.zeros((head_count, tok_rows), jnp.float32),
        jnp.zeros((tok_rows, head_count, V), jnp.float32),
    )
    state = start_state
    latent_piece = lax.all_gather(latent, "sp", axis=0, tiled=True)
    pos_piece = lax.all_gather(key_rot, "sp", axis=0, tiled=True)
    piece_len = latent_piece.shape[0]
    block_len = math.gcd(piece_len, 512)
    block_count = piece_len // block_len

    def one_block(inner, items):
        latent_rows, pos_rows = items
        key_plain = (
            jnp.dot(latent_rows, key_up, preferred_element_type=jnp.float32)
            .astype(jnp.bfloat16)
            .reshape(block_len, head_count, NOPE)
        )
        values = (
            jnp.dot(latent_rows, value_up, preferred_element_type=jnp.float32)
            .astype(jnp.bfloat16)
            .reshape(block_len, head_count, V)
        )
        return (attend_block(inner, key_plain, values, pos_rows), None)

    state, unused = lax.scan(
        one_block,
        state,
        (
            latent_piece.reshape(block_count, block_len, latent_piece.shape[1]),
            pos_piece.reshape(block_count, block_len, ROPE),
        ),
    )
    attended = (
        (state[2] / state[1].T[:, :, None]).astype(jnp.bfloat16).reshape(tok_rows, head_count * V)
    )
    own_start = lax.axis_index("tp") * part_rows
    mixed = lax.psum_scatter(
        jnp.dot(attended, out_weight, preferred_element_type=jnp.float32).astype(jnp.bfloat16),
        "tp",
        scatter_dimension=0,
        tiled=True,
    ).astype(jnp.float32)
    middle = lax.dynamic_slice_in_dim(resid_in, own_start, part_rows, 0).astype(jnp.float32) + mixed
    normed = rms_scale(middle, mixer_gain).astype(jnp.bfloat16)
    all_rows = lax.all_gather(normed, "tp", axis=0, tiled=True)
    gate_sum = jnp.dot(
        all_rows,
        lax.all_gather(gate_weight, "sp", axis=0, tiled=True),
        preferred_element_type=jnp.float32,
    )
    up_sum = jnp.dot(
        all_rows,
        lax.all_gather(up_weight, "sp", axis=0, tiled=True),
        preferred_element_type=jnp.float32,
    )
    hidden = (jax.nn.silu(gate_sum) * up_sum).astype(jnp.bfloat16)
    terms = jnp.dot(
        hidden,
        lax.all_gather(down_weight, "sp", axis=1, tiled=True),
        preferred_element_type=jnp.float32,
    )
    down_sum = lax.psum_scatter(
        terms.astype(jnp.bfloat16), "tp", scatter_dimension=0, tiled=True
    ).astype(jnp.float32)
    return (middle + 0.5 * down_sum).astype(jnp.bfloat16)

MESH = pl.DeviceIdType.MESH
BF = jnp.bfloat16
F32 = jnp.float32
BY_LAST = (((1,), (1,)), ((), ()))


def turn(values, cosine, sine):
    width = values.shape[-1]
    half = ROPE // 2
    lane = lax.broadcasted_iota(jnp.int32, values.shape, 1) % ROPE
    swapped = jnp.where(lane < half, pltpu.roll(values, width - half, 1), pltpu.roll(values, half, 1))
    return values * cosine + swapped * sine


def layer_kernel(
    sizes,
    latent_ref,
    shared_ref,
    inv_ref,
    lgain_ref,
    mgain_ref,
    query_hbm,
    turn_hbm,
    kup_hbm,
    vup_hbm,
    ow_hbm,
    resid_hbm,
    gate_hbm,
    up_hbm,
    down_hbm,
    out_ref,
    query_ref,
    turn_ref,
    kup_ref,
    vup_ref,
    ow_ref,
    resid_ref,
    raw_buf,
    wt_buf,
    kv_buf,
    key_buf,
    val_buf,
    att_buf,
    mix_buf,
    mixb_buf,
    mixr_buf,
    mid_buf,
    w_buf,
    wd_buf,
    n_buf,
    h_buf,
    acc_buf,
    r_buf,
    load_sem,
    l_ssem,
    l_rsem,
    f_ssem,
    f_rsem,
    m_ssem,
    m_rsem,
    w_ssem,
    w_rsem,
    x_ssem,
    x_rsem,
    a_ssem,
    a_rsem,
    s_ssem,
    s_rsem,
):
    sp, tp = sizes
    s = lax.axis_index("sp")
    t = lax.axis_index("tp")
    core = t % 2
    x = t // 2
    y = s % 2
    zl = (s // 2) % 2
    zh = s // 4
    other = t + 1 - 2 * core
    rows = latent_ref.shape[0]
    half_rows = rows // 2
    part = rows // tp
    hid, cols = down_hbm.shape[1:]
    kv_width = latent_ref.shape[1]
    lanes = cols // 2

    def ring(q):
        flip = lambda bit, by: bit + by * (1 - 2 * bit)
        return flip(zh, q // 4) * 4 + flip(zl, q // 2 % 2) * 2 + flip(y, q % 2)

    def remote(src, dst, ssem, rsem, dev):
        return pltpu.make_async_remote_copy(
            src_ref=src, dst_ref=dst, send_sem=ssem, recv_sem=rsem, device_id=dev, device_id_type=MESH
        )

    sends = []

    def send(src, dst, ssem, rsem, dev):
        cp = remote(src, dst, ssem, rsem, dev)
        cp.start()
        sends.append(cp)

    def arrived(ref, rsem):
        remote(ref, ref, rsem, rsem, (s, other)).wait_recv()

    barrier = pltpu.get_barrier_semaphore()
    for q in range(1, sp):
        pl.semaphore_signal(barrier, inc=1, device_id=(ring(q), t), device_id_type=MESH)
    for j in range(1, tp):
        pl.semaphore_signal(barrier, inc=1, device_id=(s, (t + j) % tp), device_id_type=MESH)

    own_rows = pl.ds(pl.multiple_of(t * part, part), part)
    own_cols = pl.ds(pl.multiple_of(s * cols, cols), cols)
    own_lanes = pl.ds(pl.multiple_of(s * lanes, lanes), lanes)
    loads = [
        pltpu.make_async_copy(src, dst, load_sem.at[i])
        for i, (src, dst) in enumerate(
            [
                (gate_hbm, raw_buf.at[0]),
                (up_hbm, raw_buf.at[1]),
                (kup_hbm, kup_ref),
                (vup_hbm, vup_ref),
                (turn_hbm, turn_ref),
                (query_hbm, query_ref),
                (ow_hbm, ow_ref),
                (resid_hbm.at[own_rows], resid_ref),
                (down_hbm.at[s, :, :lanes], wd_buf.at[0, core, :, own_lanes]),
                (down_hbm.at[s, :, lanes:], wd_buf.at[1, core, :, own_lanes]),
            ]
        )
    ]
    for load in loads:
        load.start()

    position = (s * rows + lax.broadcasted_iota(jnp.int32, (rows, 128), 0)).astype(F32)
    angles = position * inv_ref[...]
    sign = jnp.where(lax.broadcasted_iota(jnp.int32, (rows, 128), 1) % ROPE < ROPE // 2, -1.0, 1.0)
    cosine = jnp.cos(angles)
    sine = jnp.sin(angles) * sign
    lat = latent_ref[...].astype(F32)
    lat = lat * lax.rsqrt(jnp.mean(lat * lat, axis=-1, keepdims=True) + 1e-06) * lgain_ref[...]
    own_lat = lat.astype(BF)
    shared = shared_ref[...].astype(F32)
    shared = jnp.concatenate([shared] * (128 // ROPE), axis=0).T
    own_key = turn(shared, cosine, sine).astype(BF)
    for half in range(2):
        part_of = slice(half * half_rows, (half + 1) * half_rows)
        kv_buf[0, half, :, :kv_width] = own_lat[part_of]
        kv_buf[0, half, :, kv_width:] = own_key[part_of]

    pl.semaphore_wait(barrier, sp - 1 + tp - 1)

    def send_latent(slot, by):
        to = slot + by
        send(kv_buf.at[slot, core], kv_buf.at[to, core], l_ssem.at[to], l_rsem.at[to], (ring(by), t))

    for by in (4, 6, 2, 1):
        send_latent(0, by)

    for which in range(2):
        loads[which].wait()
        for j in range(raw_buf.shape[2] // 128):
            tile = slice(j * 128, (j + 1) * 128)
            wt_buf[which, tile, :] = raw_buf[which, :, tile].T

    def hid_rows(dest):
        return pl.ds(pl.multiple_of(dest * hid, 16), hid)

    def weight_slot(which, lane_of, side=core):
        if which < 2:
            return w_buf.at[which, side, :, pl.ds(pl.multiple_of(lane_of * cols, cols), cols)]
        return wd_buf.at[which - 2, side, :, pl.ds(pl.multiple_of(lane_of * lanes, lanes), lanes)]

    def send_weights(some):
        for which, q in some:
            dest = ring(q)
            if which < 2:
                src = wt_buf.at[which, hid_rows(dest), :]
            else:
                src = down_hbm.at[dest, :, (which - 2) * lanes:(which - 1) * lanes]
            send(src, weight_slot(which, s), w_ssem.at[which, q], w_rsem.at[which, q], (dest, t))

    def pass_weights(some):
        for which, q in some:
            slot = weight_slot(which, ring(q))
            if q:
                arrived(slot, w_rsem.at[which, q])
            send(slot, slot, x_ssem.at[which, q], x_rsem.at[which, q], (s, other))

    def passed_weights(which):
        for q in range(sp):
            arrived(weight_slot(which, ring(q), 1 - core), x_rsem.at[which, q])

    near = [(w, q) for q in (1, 3, 2) for w in range(2)]
    far = [(w, q) for q in (7, 5, 6, 4) for w in range(2)]
    first = far[:2] + near[:2] + far[2:3] + near[2:3] + far[3:4] + near[3:4] + far[4:5]
    second = far[5:6]
    third = far[6:7] + near[4:5] + far[7:] + near[5:]
    fourth = [(w, q) for w in (2, 3) for q in (7, 5, 6, 4, 3, 2, 1)]

    send_weights(first)
    for which in range(2):
        w_buf[which, core, :, own_cols] = wt_buf[which, hid_rows(s), :]

    def make_kv(k):
        piece = kv_buf[k].reshape(rows, kv_buf.shape[3])
        piece_lat = piece[:, :kv_width]
        key_buf[k * rows:(k + 1) * rows, :] = jnp.dot(
            piece_lat, kup_ref[...], preferred_element_type=F32
        ).astype(BF)
        val_buf[k * rows:(k + 1) * rows, :] = jnp.dot(
            piece_lat, vup_ref[...], preferred_element_type=F32
        ).astype(BF)

    for load in loads[2:]:
        load.wait()
    make_kv(0)
    query_rot = turn(
        turn_ref[...].astype(F32),
        jnp.concatenate([cosine] * (turn_ref.shape[1] // 128), axis=1),
        jnp.concatenate([sine] * (turn_ref.shape[1] // 128), axis=1),
    ).astype(BF)

    def pass_latent(slot):
        send(kv_buf.at[slot, core], kv_buf.at[slot, core], f_ssem.at[slot], f_rsem.at[slot], (s, other))

    for slot in (2, 4, 6, 1, 3, 5, 7):
        arrived(kv_buf.at[slot, core], l_rsem.at[slot])
        if slot % 2 == 0:
            send_latent(slot, 1)
        pass_latent(slot)
    for slot in (2, 4, 6, 1, 3, 5, 7):
        arrived(kv_buf.at[slot, 1 - core], f_rsem.at[slot])
        make_kv(slot)

    scale = (NOPE + ROPE) ** (-0.5)
    all_rot = kv_buf[...].reshape(sp * rows, kv_buf.shape[3])[:, kv_width:]
    lane = lax.broadcasted_iota(jnp.int32, (rows, 128), 1)
    for pair in range(query_ref.shape[1] // 128):
        span = slice(pair * 128, (pair + 1) * 128)
        keys = jnp.concatenate([key_buf[:, span], all_rot], axis=1)
        vals = val_buf[:, span]
        results = []
        for inner in range(2):
            head = pair * 2 + inner
            tile = head * ROPE // 128
            group = head % (128 // ROPE)
            q_plain = jnp.where(lane // NOPE == inner, query_ref[:, span], jnp.zeros((), BF))
            q_turn = jnp.where(
                lane // ROPE == group, query_rot[:, tile * 128:(tile + 1) * 128], jnp.zeros((), BF)
            )
            score = lax.dot_general(
                jnp.concatenate([q_plain, q_turn], axis=1), keys, BY_LAST, preferred_element_type=F32
            ) * scale
            top = jnp.max(score, axis=-1, keepdims=True)
            expo = jnp.exp(score - top)
            total = jnp.sum(expo, axis=-1, keepdims=True)
            results.append(jnp.dot(expo.astype(BF), vals, preferred_element_type=F32) / total)
        att_buf[:, span] = jnp.where(lane < V, results[0], results[1]).astype(BF)

    mix_buf[...] = jnp.dot(att_buf[...], ow_ref[...], preferred_element_type=F32)
    mixb_buf[...] = mix_buf[...].astype(BF).reshape(mixb_buf.shape)
    for j in range(1, tp):
        dest = (t + j) % tp
        send(mixb_buf.at[dest], mixr_buf.at[j], m_ssem.at[j], m_rsem.at[j], (s, dest))
    mid = resid_ref[...].astype(F32) + mix_buf[own_rows, :]
    for j in range(1, tp):
        arrived(mixr_buf.at[j], m_rsem.at[j])
        mid = mid + mixr_buf[j].astype(F32)
    mid_buf[...] = mid
    normed = mid * lax.rsqrt(jnp.mean(mid * mid, axis=-1, keepdims=True) + 1e-06) * mgain_ref[...]
    n_buf[0] = normed.astype(BF)

    a_x = 1 - core
    along_x = ((s, (1 - x) * 2 + core))
    along_y = (ring(1), t)
    pick = lambda first_x, i: first_x * along_x[i] + (1 - first_x) * along_y[i]
    steps = (
        (8, (pick(a_x, 0), pick(a_x, 1))),
        (4, (pick(core, 0), pick(core, 1))),
        (2, (ring(2), t)),
        (1, (ring(4), t)),
    )

    def spread(slot):
        for by, dev in reversed(steps):
            if by > slot:
                to = slot + by
                send(n_buf.at[slot], n_buf.at[to], a_ssem.at[to], a_rsem.at[to], dev)

    spread(0)
    send_weights(second)
    arrived(n_buf.at[1], a_rsem.at[1])
    spread(1)
    send_weights(third)
    for slot in (2, 3):
        arrived(n_buf.at[slot], a_rsem.at[slot])
        spread(slot)
    send_weights(fourth)
    for slot in (4, 5, 6, 7):
        arrived(n_buf.at[slot], a_rsem.at[slot])
        spread(slot)
    pass_weights([(w, 0) for w in range(2)] + first + second + third)
    for slot in range(8, 16):
        arrived(n_buf.at[slot], a_rsem.at[slot])
    passed_weights(0)
    passed_weights(1)

    group = n_buf.shape[0] // 2
    gate_w = w_buf[0].reshape(2 * hid, w_buf.shape[3])
    up_w = w_buf[1].reshape(2 * hid, w_buf.shape[3])
    for g in range(2):
        block = n_buf[g * group:(g + 1) * group].reshape(group * part, n_buf.shape[2])
        gate = lax.dot_general(block, gate_w, BY_LAST, preferred_element_type=F32)
        up = lax.dot_general(block, up_w, BY_LAST, preferred_element_type=F32)
        h_buf[g * group * part:(g + 1) * group * part, :] = (gate / (1.0 + jnp.exp(-gate)) * up).astype(BF)

    def sums(h, slot, count):
        by, dev = next(step for step in steps if slot >= step[0])
        some = pl.ds(slot, count)
        send(acc_buf.at[h, some], r_buf.at[h, some], s_ssem.at[h, slot], s_rsem.at[h, slot], dev)

    def project(h):
        weights = wd_buf[h].reshape(2 * hid, wd_buf.shape[3])
        for g in (1, 0):
            down = jnp.dot(
                h_buf[g * group * part:(g + 1) * group * part, :], weights, preferred_element_type=F32
            )
            acc_buf[h, g * group:(g + 1) * group] = down.astype(BF).reshape(
                group, part, acc_buf.shape[3]
            )
            if g:
                for slot in (14, 12, 10, 8):
                    sums(h, slot, 2)

    def join(h, slot, count, by):
        some = slice(slot + by, slot + by + count)
        arrived(r_buf.at[h, pl.ds(slot + by, count)], s_rsem.at[h, slot + by])
        acc_buf[h, slot:slot + count] = (
            acc_buf[h, slot:slot + count].astype(F32) + r_buf[h, some].astype(F32)
        ).astype(BF)

    def reduce_first(h):
        for slot in (6, 4):
            join(h, slot, 2, 8)
            sums(h, slot, 2)

    def reduce_second(h):
        join(h, 2, 2, 8)
        join(h, 2, 2, 4)
        sums(h, 2, 2)

    def reduce_third(h):
        join(h, 0, 2, 8)
        join(h, 0, 2, 4)
        join(h, 0, 2, 2)
        sums(h, 1, 1)

    def finish(h):
        arrived(r_buf.at[h, pl.ds(1, 1)], s_rsem.at[h, 1])
        value = acc_buf[h, 0].astype(F32) + r_buf[h, 1].astype(F32)
        for k in range(sp):
            span = slice(k * cols + h * lanes, k * cols + (h + 1) * lanes)
            out_ref[:, span] = (
                mid_buf[:, span] + 0.5 * value[:, k * lanes:(k + 1) * lanes]
            ).astype(BF)

    down_part = [[(w, q) for q in range(sp)] for w in (2, 3)]
    pass_weights(down_part[0])
    passed_weights(2)
    project(0)
    reduce_first(0)
    pass_weights(down_part[1])
    reduce_second(0)
    passed_weights(3)
    project(1)
    reduce_third(0)
    reduce_first(1)
    reduce_second(1)
    finish(0)
    reduce_third(1)
    finish(1)

    for cp in sends:
        cp.wait_send()


def fused_layer(
    resid_in,
    query_plain,
    query_turn,
    latent_raw,
    shared_key,
    latent_gain,
    key_up,
    value_up,
    out_weight,
    mixer_gain,
    gate_weight,
    up_weight,
    down_weight,
):
    sp = lax.axis_size("sp")
    tp = lax.axis_size("tp")
    rows, width = resid_in.shape
    part = rows // tp
    hid = down_weight.shape[0] // sp
    cols = down_weight.shape[1]
    kv = latent_raw.shape[1]
    heads_width = query_plain.shape[1]
    inverse = 10000.0 ** (-jnp.arange(0, ROPE, 2, dtype=F32) / ROPE)
    inverse_lanes = jnp.tile(inverse, 128 * 2 // ROPE)[None, :]
    chips = sp * tp // 2
    dma = pltpu.SemaphoreType.DMA
    vmem = lambda *shape: pltpu.VMEM(shape, BF)
    near = pl.BlockSpec(memory_space=pltpu.VMEM)
    far = pl.BlockSpec(memory_space=pl.ANY)
    return pl.pallas_call(
        functools.partial(layer_kernel, (sp, tp)),
        out_shape=jax.ShapeDtypeStruct((part, width), BF),
        in_specs=[near] * 5 + [far] * 9,
        out_specs=near,
        scratch_shapes=[
            vmem(*query_plain.shape),
            vmem(*query_turn.shape),
            vmem(*key_up.shape),
            vmem(*value_up.shape),
            vmem(*out_weight.shape),
            vmem(part, width),
            vmem(2, *gate_weight.shape),
            vmem(2, *gate_weight.shape[::-1]),
            vmem(sp, 2, rows // 2, kv + 128),
            vmem(sp * rows, heads_width),
            vmem(sp * rows, heads_width),
            vmem(rows, heads_width),
            pltpu.VMEM((rows, width), F32),
            vmem(tp, part, width),
            vmem(tp, part, width),
            pltpu.VMEM((part, width), F32),
            vmem(2, 2, hid, width),
            vmem(2, 2, hid, width // 2),
            vmem(chips, part, width),
            vmem(chips * part, 2 * hid),
            vmem(2, chips, part, width // 2),
            vmem(2, chips, part, width // 2),
            dma((10,)),
            dma((sp,)),
            dma((sp,)),
            dma((sp,)),
            dma((sp,)),
            dma((tp,)),
            dma((tp,)),
            dma((4, sp)),
            dma((4, sp)),
            dma((4, sp)),
            dma((4, sp)),
            dma((chips,)),
            dma((chips,)),
            dma((2, chips)),
            dma((2, chips)),
        ],
        compiler_params=pltpu.CompilerParams(
            collective_id=0, has_side_effects=True, vmem_limit_bytes=60 * 1024 * 1024
        ),
    )(
        latent_raw,
        shared_key.T,
        inverse_lanes,
        latent_gain[None, :],
        mixer_gain[None, :],
        query_plain,
        query_turn,
        key_up,
        value_up,
        out_weight,
        resid_in,
        gate_weight,
        up_weight,
        down_weight.reshape(sp, hid, cols),
    )


def per_device(*arrays):
    resid_in, query_plain, query_turn, latent_raw = arrays[:4]
    down_weight = arrays[-1]
    sp = lax.axis_size("sp")
    tp = lax.axis_size("tp")
    rows = resid_in.shape[0]
    fits = (
        sp // 4 == 2
        and tp // 2 == 2
        and rows % (32 * tp) == 0
        and down_weight.shape[0] % (16 * sp) == 0
        and down_weight.shape[1] % 128 == 0
        and latent_raw.shape[1] % 128 == 0
        and query_plain.shape[1] % 128 == 0
        and query_turn.shape[1] % 128 == 0
        and rows * sp <= 1024
        and sp * tp <= 32
    )
    if fits:
        return fused_layer(*arrays)
    return plain_layer(*arrays)


def solution(mesh):
    return jax.shard_map(
        per_device,
        mesh=mesh,
        in_specs=(
            P("sp", None),
            P("sp", "tp"),
            P("sp", "tp"),
            P("sp", None),
            P("sp", None),
            P(),
            P(None, "tp"),
            P(None, "tp"),
            P("tp", None),
            P(),
            P("sp", "tp"),
            P("sp", "tp"),
            P("tp", "sp"),
        ),
        out_specs=P(("sp", "tp"), None),
        check_vma=False,
    )
```

```python
import functools
import math

import jax
import jax.numpy as jnp
from jax import lax
from jax.experimental import pallas as pl
from jax.experimental.pallas import tpu as pltpu
from jax.sharding import PartitionSpec as P

NOPE = 64
ROPE = 32
V = 64


def rotate(values, cosine, sine):
    half_width = values.shape[-1] // 2
    first = values[..., :half_width]
    second = values[..., half_width:]
    return jnp.concatenate(
        [first * cosine - second * sine, first * sine + second * cosine], axis=-1
    )


def rms_scale(values, gain):
    return values * lax.rsqrt(jnp.mean(values * values, axis=-1, keepdims=True) + 1e-06) * gain


def plain_layer(
    resid_in,
    query_plain,
    query_turn,
    latent_raw,
    shared_key,
    latent_gain,
    key_up,
    value_up,
    out_weight,
    mixer_gain,
    gate_weight,
    up_weight,
    down_weight,
):
    tok_rows = resid_in.shape[0]
    head_count = query_plain.shape[1] // NOPE
    part_rows = tok_rows // lax.axis_size("tp")
    offset = lax.axis_index("sp") * tok_rows
    position = (offset + jnp.arange(tok_rows, dtype=jnp.int32)).astype(jnp.float32)
    inverse = 10000.0 ** (-jnp.arange(0, ROPE, 2, dtype=jnp.float32) / ROPE)
    angles = position[:, None] * inverse[None, :]
    cosine = jnp.cos(angles)
    sine = jnp.sin(angles)
    query_heads = query_plain.reshape(tok_rows, head_count, NOPE)
    query_rot = rotate(
        query_turn.reshape(tok_rows, head_count, ROPE).astype(jnp.float32),
        cosine[:, None, :],
        sine[:, None, :],
    ).astype(jnp.bfloat16)
    latent = rms_scale(latent_raw.astype(jnp.float32), latent_gain).astype(jnp.bfloat16)
    key_rot = rotate(shared_key.astype(jnp.float32), cosine, sine).astype(jnp.bfloat16)
    softmax_scale = (NOPE + ROPE) ** (-0.5)

    def attend_block(state, key_plain, values, key_pos):
        run_max, run_total, run_acc = state
        score = jnp.einsum(
            "qhd,khd->hqk", query_heads, key_plain, preferred_element_type=jnp.float32
        )
        score = score + jnp.einsum(
            "qhr,kr->hqk", query_rot, key_pos, preferred_element_type=jnp.float32
        )
        score = score * softmax_scale
        new_max = jnp.maximum(run_max, jnp.max(score, axis=-1))
        shrink = jnp.exp(run_max - new_max)
        expo = jnp.exp(score - new_max[:, :, None])
        run_total = run_total * shrink + jnp.sum(expo, axis=-1)
        run_acc = run_acc * shrink.T[:, :, None] + jnp.einsum(
            "hqk,khd->qhd", expo.astype(jnp.bfloat16), values, preferred_element_type=jnp.float32
        )
        return (new_max, run_total, run_acc)

    start_state = (
        jnp.full((head_count, tok_rows), -jnp.inf, jnp.float32),
        jnp.zeros((head_count, tok_rows), jnp.float32),
        jnp.zeros((tok_rows, head_count, V), jnp.float32),
    )
    state = start_state
    latent_piece = lax.all_gather(latent, "sp", axis=0, tiled=True)
    pos_piece = lax.all_gather(key_rot, "sp", axis=0, tiled=True)
    piece_len = latent_piece.shape[0]
    block_len = math.gcd(piece_len, 512)
    block_count = piece_len // block_len

    def one_block(inner, items):
        latent_rows, pos_rows = items
        key_plain = (
            jnp.dot(latent_rows, key_up, preferred_element_type=jnp.float32)
            .astype(jnp.bfloat16)
            .reshape(block_len, head_count, NOPE)
        )
        values = (
            jnp.dot(latent_rows, value_up, preferred_element_type=jnp.float32)
            .astype(jnp.bfloat16)
            .reshape(block_len, head_count, V)
        )
        return (attend_block(inner, key_plain, values, pos_rows), None)

    state, unused = lax.scan(
        one_block,
        state,
        (
            latent_piece.reshape(block_count, block_len, latent_piece.shape[1]),
            pos_piece.reshape(block_count, block_len, ROPE),
        ),
    )
    attended = (
        (state[2] / state[1].T[:, :, None]).astype(jnp.bfloat16).reshape(tok_rows, head_count * V)
    )
    own_start = lax.axis_index("tp") * part_rows
    mixed = lax.psum_scatter(
        jnp.dot(attended, out_weight, preferred_element_type=jnp.float32).astype(jnp.bfloat16),
        "tp",
        scatter_dimension=0,
        tiled=True,
    ).astype(jnp.float32)
    middle = lax.dynamic_slice_in_dim(resid_in, own_start, part_rows, 0).astype(jnp.float32) + mixed
    normed = rms_scale(middle, mixer_gain).astype(jnp.bfloat16)
    all_rows = lax.all_gather(normed, "tp", axis=0, tiled=True)
    gate_sum = jnp.dot(
        all_rows,
        lax.all_gather(gate_weight, "sp", axis=0, tiled=True),
        preferred_element_type=jnp.float32,
    )
    up_sum = jnp.dot(
        all_rows,
        lax.all_gather(up_weight, "sp", axis=0, tiled=True),
        preferred_element_type=jnp.float32,
    )
    hidden = (jax.nn.silu(gate_sum) * up_sum).astype(jnp.bfloat16)
    terms = jnp.dot(
        hidden,
        lax.all_gather(down_weight, "sp", axis=1, tiled=True),
        preferred_element_type=jnp.float32,
    )
    down_sum = lax.psum_scatter(
        terms.astype(jnp.bfloat16), "tp", scatter_dimension=0, tiled=True
    ).astype(jnp.float32)
    return (middle + 0.5 * down_sum).astype(jnp.bfloat16)

MESH = pl.DeviceIdType.MESH
BF = jnp.bfloat16
F32 = jnp.float32
BY_LAST = (((1,), (1,)), ((), ()))


def turn(values, cosine, sine):
    width = values.shape[-1]
    half = ROPE // 2
    lane = lax.broadcasted_iota(jnp.int32, values.shape, 1) % ROPE
    swapped = jnp.where(lane < half, pltpu.roll(values, width - half, 1), pltpu.roll(values, half, 1))
    return values * cosine + swapped * sine


def layer_kernel(
    sizes,
    latent_ref,
    shared_ref,
    inv_ref,
    lgain_ref,
    mgain_ref,
    query_hbm,
    turn_hbm,
    kup_hbm,
    vup_hbm,
    ow_hbm,
    resid_hbm,
    gate_hbm,
    up_hbm,
    down_hbm,
    out_ref,
    query_ref,
    turn_ref,
    kup_ref,
    vup_ref,
    ow_ref,
    resid_ref,
    raw_buf,
    wt_buf,
    relay_buf,
    kv_buf,
    key_buf,
    val_buf,
    att_buf,
    mix_buf,
    pair_buf,
    paird_buf,
    cross_buf,
    crossr_buf,
    mid_buf,
    w_buf,
    wd_buf,
    n_buf,
    h_buf,
    acc_buf,
    r_buf,
    load_sem,
    l_ssem,
    l_rsem,
    f_ssem,
    f_rsem,
    m_ssem,
    m_rsem,
    w_ssem,
    w_rsem,
    y_ssem,
    y_rsem,
    x_ssem,
    x_rsem,
    a_ssem,
    a_rsem,
    s_ssem,
    s_rsem,
):
    sp, tp = sizes
    s = lax.axis_index("sp")
    t = lax.axis_index("tp")
    core = t % 2
    x = t // 2
    y = s % 2
    zl = (s // 2) % 2
    zh = s // 4
    other = t + 1 - 2 * core
    rows = latent_ref.shape[0]
    half_rows = rows // 2
    part = rows // tp
    hid, cols = down_hbm.shape[1:]
    kv_width = latent_ref.shape[1]
    lanes = cols // 2
    width = ow_hbm.shape[1]
    along_x = (s, (1 - x) * 2 + core)

    def ring(q):
        flip = lambda bit, by: bit + by * (1 - 2 * bit)
        return flip(zh, q // 4) * 4 + flip(zl, q // 2 % 2) * 2 + flip(y, q % 2)

    def remote(src, dst, ssem, rsem, dev):
        return pltpu.make_async_remote_copy(
            src_ref=src, dst_ref=dst, send_sem=ssem, recv_sem=rsem, device_id=dev, device_id_type=MESH
        )

    def send(src, dst, ssem, rsem, dev):
        remote(src, dst, ssem, rsem, dev).start()

    def sent(ref, ssem):
        remote(ref, ref, ssem, ssem, (s, other)).wait_send()

    def arrived(ref, rsem):
        remote(ref, ref, rsem, rsem, (s, other)).wait_recv()

    barrier = pltpu.get_barrier_semaphore()
    for q in range(1, sp):
        pl.semaphore_signal(barrier, inc=1, device_id=(ring(q), t), device_id_type=MESH)
    for j in range(1, tp):
        pl.semaphore_signal(barrier, inc=1, device_id=(s, (t + j) % tp), device_id_type=MESH)

    own_rows = pl.ds(pl.multiple_of(t * part, part), part)
    own_cols = pl.ds(pl.multiple_of(s * cols, cols), cols)
    own_lanes = pl.ds(pl.multiple_of(s * lanes, lanes), lanes)
    loads = [
        pltpu.make_async_copy(src, dst, load_sem.at[i])
        for i, (src, dst) in enumerate(
            [
                (gate_hbm, raw_buf.at[0]),
                (up_hbm, raw_buf.at[1]),
                (kup_hbm, kup_ref),
                (vup_hbm, vup_ref),
                (turn_hbm, turn_ref),
                (query_hbm, query_ref),
                (ow_hbm, ow_ref),
                (resid_hbm.at[own_rows], resid_ref),
                (down_hbm.at[s, :, :lanes], wd_buf.at[0, core, :, own_lanes]),
                (down_hbm.at[s, :, lanes:], wd_buf.at[1, core, :, own_lanes]),
                (down_hbm, wt_buf.at[2]),
            ]
        )
    ]
    for load in loads:
        load.start()

    position = (s * rows + lax.broadcasted_iota(jnp.int32, (rows, 128), 0)).astype(F32)
    angles = position * inv_ref[...]
    sign = jnp.where(lax.broadcasted_iota(jnp.int32, (rows, 128), 1) % ROPE < ROPE // 2, -1.0, 1.0)
    cosine = jnp.cos(angles)
    sine = jnp.sin(angles) * sign
    lat = latent_ref[...].astype(F32)
    lat = lat * lax.rsqrt(jnp.mean(lat * lat, axis=-1, keepdims=True) + 1e-06) * lgain_ref[...]
    own_lat = lat.astype(BF)
    shared = shared_ref[...].astype(F32)
    shared = jnp.concatenate([shared] * (128 // ROPE), axis=0).T
    own_key = turn(shared, cosine, sine).astype(BF)
    for half in range(2):
        part_of = slice(half * half_rows, (half + 1) * half_rows)
        kv_buf[0, half, :, :kv_width] = own_lat[part_of]
        kv_buf[0, half, :, kv_width:] = own_key[part_of]

    pl.semaphore_wait(barrier, sp - 1 + tp - 1)

    along_y = (ring(1), t)

    def send_latent(slot, by):
        to = slot + by
        send(kv_buf.at[slot, core], kv_buf.at[to, core], l_ssem.at[0], l_rsem.at[to], (ring(by), t))

    for by in (6, 4, 2, 1):
        send_latent(0, by)

    for which in range(2):
        loads[which].wait()
        turned_buf = wt_buf.at[which].reshape(sp * hid, cols)
        for j in range(raw_buf.shape[2] // 128):
            tile = slice(j * 128, (j + 1) * 128)
            turned_buf[tile, :] = raw_buf[which, :, tile].T

    first = [(0, 6), (1, 6), (0, 4), (1, 4)]
    second = [(0, 7)]
    third = [(1, 7), (0, 5), (1, 5), (0, 2), (1, 2), (0, 3), (1, 3)]
    fourth = [(w, q) for w in (2, 3) for q in (6, 7, 4, 5, 2, 3)]

    def late(which, q):
        return int((which, q) not in first and (q != 1 or which > 1))

    def weight_slot(which, lane_of, side=core):
        if which < 2:
            return w_buf.at[which, side, :, pl.ds(pl.multiple_of(lane_of * cols, cols), cols)]
        return wd_buf.at[which - 2, side, :, pl.ds(pl.multiple_of(lane_of * lanes, lanes), lanes)]

    def lanes_of(ref, which):
        return ref if which < 2 else ref.at[:, (which - 2) * lanes:(which - 1) * lanes]

    def send_weights(some):
        for which, q in some:
            kind = min(which, 2)
            if q > 1 and q % 2:
                src, owner, dest = relay_buf.at[kind, q // 2 - 1], ring(1), (ring(q - 1), t)
            else:
                src, owner, dest = wt_buf.at[kind, ring(q)], s, (ring(q), t)
            send(
                lanes_of(src, which),
                weight_slot(which, owner),
                w_ssem.at[which],
                w_rsem.at[which, late(which, q)],
                dest,
            )

    def send_relays(kind):
        for q in (7, 5, 3):
            send(
                wt_buf.at[kind, ring(q)], relay_buf.at[kind, q // 2 - 1], y_ssem.at[kind], y_rsem.at[kind], along_y
            )
        send_weights([(which, 1) for which in ((kind,) if kind < 2 else (2, 3))])

    def relayed(kind):
        arrived(relay_buf.at[kind], y_rsem.at[kind])

    def some_of(which, side, count):
        if which < 2:
            return w_buf.at[which, side, :, :count * cols]
        return wd_buf.at[which - 2, side, :, :count * lanes]

    def pass_weights(which, group):
        some = [q for q in range(1, sp) if late(which, q) == group]
        arrived(some_of(which, core, len(some)), w_rsem.at[which, group])
        for q in some + [0] * group:
            slot = weight_slot(which, ring(q))
            send(slot, slot, x_ssem.at[which], x_rsem.at[which], (s, other))

    def passed_weights(which):
        arrived(some_of(which, 1 - core, sp), x_rsem.at[which])

    send_relays(0)
    send_relays(1)
    for which in range(2):
        w_buf[which, core, :, own_cols] = wt_buf[which, s]

    def make_kv(k):
        piece = kv_buf[k].reshape(rows, kv_buf.shape[3])
        piece_lat = piece[:, :kv_width]
        key_buf[k * rows:(k + 1) * rows, :] = jnp.dot(
            piece_lat, kup_ref[...], preferred_element_type=F32
        ).astype(BF)
        val_buf[k * rows:(k + 1) * rows, :] = jnp.dot(
            piece_lat, vup_ref[...], preferred_element_type=F32
        ).astype(BF)

    for load in loads[2:10]:
        load.wait()
    make_kv(0)
    query_rot = turn(
        turn_ref[...].astype(F32),
        jnp.concatenate([cosine] * (turn_ref.shape[1] // 128), axis=1),
        jnp.concatenate([sine] * (turn_ref.shape[1] // 128), axis=1),
    ).astype(BF)

    def pass_latent(slot):
        send(kv_buf.at[slot, core], kv_buf.at[slot, core], f_ssem.at[0], f_rsem.at[slot], (s, other))

    def take_latent(slot):
        arrived(kv_buf.at[slot, core], l_rsem.at[slot])
        pass_latent(slot)

    take_latent(1)
    for by in (6, 4, 2):
        send_latent(1, by)
    loads[10].wait()
    send_relays(2)
    order = (2, 4, 6, 3, 5, 7)
    for slot in order:
        take_latent(slot)
    send_weights(first)
    for slot in (1,) + order:
        arrived(kv_buf.at[slot, 1 - core], f_rsem.at[slot])
        make_kv(slot)

    scale = (NOPE + ROPE) ** (-0.5)
    all_rot = kv_buf[...].reshape(sp * rows, kv_buf.shape[3])[:, kv_width:]
    lane = lax.broadcasted_iota(jnp.int32, (rows, 128), 1)
    for pair in range(query_ref.shape[1] // 128):
        span = slice(pair * 128, (pair + 1) * 128)
        keys = jnp.concatenate([key_buf[:, span], all_rot], axis=1)
        vals = val_buf[:, span]
        results = []
        for inner in range(2):
            head = pair * 2 + inner
            tile = head * ROPE // 128
            group = head % (128 // ROPE)
            q_plain = jnp.where(lane // NOPE == inner, query_ref[:, span], jnp.zeros((), BF))
            q_turn = jnp.where(
                lane // ROPE == group, query_rot[:, tile * 128:(tile + 1) * 128], jnp.zeros((), BF)
            )
            score = lax.dot_general(
                jnp.concatenate([q_plain, q_turn], axis=1), keys, BY_LAST, preferred_element_type=F32
            ) * scale
            top = jnp.max(score, axis=-1, keepdims=True)
            expo = jnp.exp(score - top)
            total = jnp.sum(expo, axis=-1, keepdims=True)
            results.append(jnp.dot(expo.astype(BF), vals, preferred_element_type=F32) / total)
        att_buf[:, span] = jnp.where(lane < V, results[0], results[1]).astype(BF)

    span_of = [slice(c * width // 2, (c + 1) * width // 2) for c in range(2)]
    for c, span in enumerate(span_of):
        mix = jnp.dot(att_buf[...], ow_ref[:, span], preferred_element_type=F32)
        mix_buf[:, span] = mix
        for dest in range(tp):
            pair_buf[dest % 2, c, dest // 2] = mix[dest * part:(dest + 1) * part].astype(BF)
        send(pair_buf.at[1 - core, c], paird_buf.at[c], m_ssem.at[c], m_rsem.at[c], (s, other))
    cross_rows = pl.ds(pl.multiple_of(((1 - x) * 2 + core) * part, part), part)
    for c, span in enumerate(span_of):
        arrived(paird_buf.at[c], m_rsem.at[c])
        cross_buf[c] = (mix_buf[cross_rows, span] + paird_buf[c, 1 - x].astype(F32)).astype(BF)
        send(cross_buf.at[c], crossr_buf.at[c], m_ssem.at[2 + c], m_rsem.at[2 + c], along_x)
    mids = [
        resid_ref[:, span].astype(F32) + mix_buf[own_rows, span] + paird_buf[c, x].astype(F32)
        for c, span in enumerate(span_of)
    ]
    for c in range(2):
        arrived(crossr_buf.at[c], m_rsem.at[2 + c])
        mids[c] = mids[c] + crossr_buf[c].astype(F32)
    mid = jnp.concatenate(mids, axis=1)
    mid_buf[...] = mid
    normed = mid * lax.rsqrt(jnp.mean(mid * mid, axis=-1, keepdims=True) + 1e-06) * mgain_ref[...]
    n_buf[0] = normed.astype(BF)

    a_x = 1 - core
    pick = lambda first_x, i: first_x * along_x[i] + (1 - first_x) * along_y[i]
    steps = (
        (8, (pick(a_x, 0), pick(a_x, 1))),
        (4, (pick(core, 0), pick(core, 1))),
        (2, (ring(2), t)),
        (1, (ring(4), t)),
    )

    def spread(slot):
        for by, dev in reversed(steps):
            if by > slot:
                to = slot + by
                send(n_buf.at[slot], n_buf.at[to], a_ssem.at[0], a_rsem.at[min(to, sp)], dev)

    spread(0)
    relayed(0)
    send_weights(second)
    arrived(n_buf.at[1], a_rsem.at[1])
    spread(1)
    relayed(1)
    send_weights(third)
    for slot in (2, 3):
        arrived(n_buf.at[slot], a_rsem.at[slot])
        spread(slot)
    relayed(2)
    send_weights(fourth)
    pass_weights(0, 0)
    pass_weights(1, 0)
    for slot in (4, 5, 6, 7):
        arrived(n_buf.at[slot], a_rsem.at[slot])
        spread(slot)
    pass_weights(0, 1)
    pass_weights(1, 1)
    passed_weights(0)
    passed_weights(1)

    group = n_buf.shape[0] // 2
    gate_w = w_buf[0].reshape(2 * hid, w_buf.shape[3])
    up_w = w_buf[1].reshape(2 * hid, w_buf.shape[3])
    for g in range(2):
        if g:
            arrived(n_buf.at[pl.ds(group, group)], a_rsem.at[sp])
        block = n_buf[g * group:(g + 1) * group].reshape(group * part, n_buf.shape[2])
        gate = lax.dot_general(block, gate_w, BY_LAST, preferred_element_type=F32)
        up = lax.dot_general(block, up_w, BY_LAST, preferred_element_type=F32)
        h_buf[g * group * part:(g + 1) * group * part, :] = (gate / (1.0 + jnp.exp(-gate)) * up).astype(BF)

    def sums(h, slot, count):
        by, dev = next(step for step in steps if slot >= step[0])
        some = pl.ds(slot, count)
        send(acc_buf.at[h, some], r_buf.at[h, some], s_ssem.at[h], s_rsem.at[h, slot // 2], dev)

    def project(h):
        weights = wd_buf[h].reshape(2 * hid, wd_buf.shape[3])
        for g in (1, 0):
            down = jnp.dot(
                h_buf[g * group * part:(g + 1) * group * part, :], weights, preferred_element_type=F32
            )
            acc_buf[h, g * group:(g + 1) * group] = down.astype(BF).reshape(
                group, part, acc_buf.shape[3]
            )
            if g:
                for slot in (14, 12, 10, 8):
                    sums(h, slot, 2)

    def join(h, slot, count, by):
        some = slice(slot + by, slot + by + count)
        arrived(r_buf.at[h, pl.ds(slot + by, count)], s_rsem.at[h, (slot + by) // 2])
        acc_buf[h, slot:slot + count] = (
            acc_buf[h, slot:slot + count].astype(F32) + r_buf[h, some].astype(F32)
        ).astype(BF)

    def reduce_first(h):
        for slot in (6, 4):
            join(h, slot, 2, 8)
            sums(h, slot, 2)

    def reduce_second(h):
        join(h, 2, 2, 8)
        join(h, 2, 2, 4)
        sums(h, 2, 2)

    def reduce_third(h):
        join(h, 0, 2, 8)
        join(h, 0, 2, 4)
        join(h, 0, 2, 2)
        sums(h, 1, 1)

    def finish(h):
        arrived(r_buf.at[h, pl.ds(1, 1)], s_rsem.at[h, 0])
        value = acc_buf[h, 0].astype(F32) + r_buf[h, 1].astype(F32)
        for k in range(sp):
            span = slice(k * cols + h * lanes, k * cols + (h + 1) * lanes)
            out_ref[:, span] = (
                mid_buf[:, span] + 0.5 * value[:, k * lanes:(k + 1) * lanes]
            ).astype(BF)

    pass_weights(2, 1)
    passed_weights(2)
    project(0)
    reduce_first(0)
    pass_weights(3, 1)
    reduce_second(0)
    passed_weights(3)
    project(1)
    reduce_third(0)
    reduce_first(1)
    reduce_second(1)
    finish(0)
    reduce_third(1)
    finish(1)

    for h in range(2):
        sent(r_buf.at[h, pl.ds(1, 2 * sp - 1)], s_ssem.at[h])
    sent(n_buf.at[pl.ds(1, 2 * sp - 1)], a_ssem.at[0])
    for c in range(2):
        sent(paird_buf.at[c], m_ssem.at[c])
        sent(crossr_buf.at[c], m_ssem.at[2 + c])
    sent(kv_buf.at[pl.ds(1, sp - 1), core], l_ssem.at[0])
    sent(kv_buf.at[pl.ds(1, sp - 1), core], f_ssem.at[0])
    for kind in range(3):
        sent(relay_buf.at[kind], y_ssem.at[kind])
    for which in range(4):
        sent(some_of(which, core, sp - 1), w_ssem.at[which])
        sent(some_of(which, core, sp), x_ssem.at[which])


def fused_layer(
    resid_in,
    query_plain,
    query_turn,
    latent_raw,
    shared_key,
    latent_gain,
    key_up,
    value_up,
    out_weight,
    mixer_gain,
    gate_weight,
    up_weight,
    down_weight,
):
    sp = lax.axis_size("sp")
    tp = lax.axis_size("tp")
    rows, width = resid_in.shape
    part = rows // tp
    hid = down_weight.shape[0] // sp
    cols = down_weight.shape[1]
    kv = latent_raw.shape[1]
    heads_width = query_plain.shape[1]
    inverse = 10000.0 ** (-jnp.arange(0, ROPE, 2, dtype=F32) / ROPE)
    inverse_lanes = jnp.tile(inverse, 128 * 2 // ROPE)[None, :]
    chips = sp * tp // 2
    dma = pltpu.SemaphoreType.DMA
    vmem = lambda *shape: pltpu.VMEM(shape, BF)
    near = pl.BlockSpec(memory_space=pltpu.VMEM)
    far = pl.BlockSpec(memory_space=pl.ANY)
    return pl.pallas_call(
        functools.partial(layer_kernel, (sp, tp)),
        out_shape=jax.ShapeDtypeStruct((part, width), BF),
        in_specs=[near] * 5 + [far] * 9,
        out_specs=near,
        scratch_shapes=[
            vmem(*query_plain.shape),
            vmem(*query_turn.shape),
            vmem(*key_up.shape),
            vmem(*value_up.shape),
            vmem(*out_weight.shape),
            vmem(part, width),
            vmem(2, *gate_weight.shape),
            vmem(3, sp, hid, cols),
            vmem(3, sp // 2 - 1, hid, cols),
            vmem(sp, 2, rows // 2, kv + 128),
            vmem(sp * rows, heads_width),
            vmem(sp * rows, heads_width),
            vmem(rows, heads_width),
            pltpu.VMEM((rows, width), F32),
            vmem(2, 2, tp // 2, part, width // 2),
            vmem(2, tp // 2, part, width // 2),
            vmem(2, part, width // 2),
            vmem(2, part, width // 2),
            pltpu.VMEM((part, width), F32),
            vmem(2, 2, hid, width),
            vmem(2, 2, hid, width // 2),
            vmem(chips, part, width),
            vmem(chips * part, 2 * hid),
            vmem(2, chips, part, width // 2),
            vmem(2, chips, part, width // 2),
            dma((11,)),
            dma((1,)),
            dma((sp,)),
            dma((1,)),
            dma((sp,)),
            dma((4,)),
            dma((4,)),
            dma((4,)),
            dma((4, 2)),
            dma((3,)),
            dma((3,)),
            dma((4,)),
            dma((4,)),
            dma((1,)),
            dma((sp + 1,)),
            dma((2,)),
            dma((2, sp)),
        ],
        compiler_params=pltpu.CompilerParams(
            collective_id=0, has_side_effects=True, vmem_limit_bytes=60 * 1024 * 1024
        ),
    )(
        latent_raw,
        shared_key.T,
        inverse_lanes,
        latent_gain[None, :],
        mixer_gain[None, :],
        query_plain,
        query_turn,
        key_up,
        value_up,
        out_weight,
        resid_in,
        gate_weight,
        up_weight,
        down_weight.reshape(sp, hid, cols),
    )


def per_device(*arrays):
    resid_in, query_plain, query_turn, latent_raw = arrays[:4]
    down_weight = arrays[-1]
    sp = lax.axis_size("sp")
    tp = lax.axis_size("tp")
    rows = resid_in.shape[0]
    fits = (
        sp // 4 == 2
        and tp // 2 == 2
        and rows % (32 * tp) == 0
        and down_weight.shape[0] % (16 * sp) == 0
        and down_weight.shape[1] % 128 == 0
        and latent_raw.shape[1] % 128 == 0
        and query_plain.shape[1] % 128 == 0
        and query_turn.shape[1] % 128 == 0
        and rows * sp <= 1024
        and sp * tp <= 32
    )
    if fits:
        return fused_layer(*arrays)
    return plain_layer(*arrays)


def solution(mesh):
    return jax.shard_map(
        per_device,
        mesh=mesh,
        in_specs=(
            P("sp", None),
            P("sp", "tp"),
            P("sp", "tp"),
            P("sp", None),
            P("sp", None),
            P(),
            P(None, "tp"),
            P(None, "tp"),
            P("tp", None),
            P(),
            P("sp", "tp"),
            P("sp", "tp"),
            P("tp", "sp"),
        ),
        out_specs=P(("sp", "tp"), None),
        check_vma=False,
    )
```

```python
import functools
import math

import jax
import jax.numpy as jnp
from jax import lax
from jax.experimental import pallas as pl
from jax.experimental.pallas import tpu as pltpu
from jax.sharding import PartitionSpec as P

NOPE = 64
ROPE = 32
V = 64


def rotate(values, cosine, sine):
    half_width = values.shape[-1] // 2
    first = values[..., :half_width]
    second = values[..., half_width:]
    return jnp.concatenate(
        [first * cosine - second * sine, first * sine + second * cosine], axis=-1
    )


def rms_scale(values, gain):
    return values * lax.rsqrt(jnp.mean(values * values, axis=-1, keepdims=True) + 1e-06) * gain


def plain_layer(
    resid_in,
    query_plain,
    query_turn,
    latent_raw,
    shared_key,
    latent_gain,
    key_up,
    value_up,
    out_weight,
    mixer_gain,
    gate_weight,
    up_weight,
    down_weight,
):
    tok_rows = resid_in.shape[0]
    head_count = query_plain.shape[1] // NOPE
    part_rows = tok_rows // lax.axis_size("tp")
    offset = lax.axis_index("sp") * tok_rows
    position = (offset + jnp.arange(tok_rows, dtype=jnp.int32)).astype(jnp.float32)
    inverse = 10000.0 ** (-jnp.arange(0, ROPE, 2, dtype=jnp.float32) / ROPE)
    angles = position[:, None] * inverse[None, :]
    cosine = jnp.cos(angles)
    sine = jnp.sin(angles)
    query_heads = query_plain.reshape(tok_rows, head_count, NOPE)
    query_rot = rotate(
        query_turn.reshape(tok_rows, head_count, ROPE).astype(jnp.float32),
        cosine[:, None, :],
        sine[:, None, :],
    ).astype(jnp.bfloat16)
    latent = rms_scale(latent_raw.astype(jnp.float32), latent_gain).astype(jnp.bfloat16)
    key_rot = rotate(shared_key.astype(jnp.float32), cosine, sine).astype(jnp.bfloat16)
    softmax_scale = (NOPE + ROPE) ** (-0.5)

    def attend_block(state, key_plain, values, key_pos):
        run_max, run_total, run_acc = state
        score = jnp.einsum(
            "qhd,khd->hqk", query_heads, key_plain, preferred_element_type=jnp.float32
        )
        score = score + jnp.einsum(
            "qhr,kr->hqk", query_rot, key_pos, preferred_element_type=jnp.float32
        )
        score = score * softmax_scale
        new_max = jnp.maximum(run_max, jnp.max(score, axis=-1))
        shrink = jnp.exp(run_max - new_max)
        expo = jnp.exp(score - new_max[:, :, None])
        run_total = run_total * shrink + jnp.sum(expo, axis=-1)
        run_acc = run_acc * shrink.T[:, :, None] + jnp.einsum(
            "hqk,khd->qhd", expo.astype(jnp.bfloat16), values, preferred_element_type=jnp.float32
        )
        return (new_max, run_total, run_acc)

    start_state = (
        jnp.full((head_count, tok_rows), -jnp.inf, jnp.float32),
        jnp.zeros((head_count, tok_rows), jnp.float32),
        jnp.zeros((tok_rows, head_count, V), jnp.float32),
    )
    state = start_state
    latent_piece = lax.all_gather(latent, "sp", axis=0, tiled=True)
    pos_piece = lax.all_gather(key_rot, "sp", axis=0, tiled=True)
    piece_len = latent_piece.shape[0]
    block_len = math.gcd(piece_len, 512)
    block_count = piece_len // block_len

    def one_block(inner, items):
        latent_rows, pos_rows = items
        key_plain = (
            jnp.dot(latent_rows, key_up, preferred_element_type=jnp.float32)
            .astype(jnp.bfloat16)
            .reshape(block_len, head_count, NOPE)
        )
        values = (
            jnp.dot(latent_rows, value_up, preferred_element_type=jnp.float32)
            .astype(jnp.bfloat16)
            .reshape(block_len, head_count, V)
        )
        return (attend_block(inner, key_plain, values, pos_rows), None)

    state, unused = lax.scan(
        one_block,
        state,
        (
            latent_piece.reshape(block_count, block_len, latent_piece.shape[1]),
            pos_piece.reshape(block_count, block_len, ROPE),
        ),
    )
    attended = (
        (state[2] / state[1].T[:, :, None]).astype(jnp.bfloat16).reshape(tok_rows, head_count * V)
    )
    own_start = lax.axis_index("tp") * part_rows
    mixed = lax.psum_scatter(
        jnp.dot(attended, out_weight, preferred_element_type=jnp.float32).astype(jnp.bfloat16),
        "tp",
        scatter_dimension=0,
        tiled=True,
    ).astype(jnp.float32)
    middle = lax.dynamic_slice_in_dim(resid_in, own_start, part_rows, 0).astype(jnp.float32) + mixed
    normed = rms_scale(middle, mixer_gain).astype(jnp.bfloat16)
    all_rows = lax.all_gather(normed, "tp", axis=0, tiled=True)
    gate_sum = jnp.dot(
        all_rows,
        lax.all_gather(gate_weight, "sp", axis=0, tiled=True),
        preferred_element_type=jnp.float32,
    )
    up_sum = jnp.dot(
        all_rows,
        lax.all_gather(up_weight, "sp", axis=0, tiled=True),
        preferred_element_type=jnp.float32,
    )
    hidden = (jax.nn.silu(gate_sum) * up_sum).astype(jnp.bfloat16)
    terms = jnp.dot(
        hidden,
        lax.all_gather(down_weight, "sp", axis=1, tiled=True),
        preferred_element_type=jnp.float32,
    )
    down_sum = lax.psum_scatter(
        terms.astype(jnp.bfloat16), "tp", scatter_dimension=0, tiled=True
    ).astype(jnp.float32)
    return (middle + 0.5 * down_sum).astype(jnp.bfloat16)

MESH = pl.DeviceIdType.MESH
BF = jnp.bfloat16
F32 = jnp.float32
BY_LAST = (((1,), (1,)), ((), ()))


def turn(values, cosine, sine):
    width = values.shape[-1]
    half = ROPE // 2
    lane = lax.broadcasted_iota(jnp.int32, values.shape, 1) % ROPE
    swapped = jnp.where(lane < half, pltpu.roll(values, width - half, 1), pltpu.roll(values, half, 1))
    return values * cosine + swapped * sine


def layer_kernel(
    sizes,
    latent_ref,
    shared_ref,
    inv_ref,
    lgain_ref,
    mgain_ref,
    query_hbm,
    turn_hbm,
    kup_hbm,
    vup_hbm,
    ow_hbm,
    resid_hbm,
    gate_hbm,
    up_hbm,
    down_hbm,
    out_ref,
    query_ref,
    turn_ref,
    kup_ref,
    vup_ref,
    ow_ref,
    resid_ref,
    raw_buf,
    wt_buf,
    relay_buf,
    kv_buf,
    key_buf,
    val_buf,
    att_buf,
    mix_buf,
    pair_buf,
    paird_buf,
    cross_buf,
    crossr_buf,
    mid_buf,
    w_buf,
    wd_buf,
    n_buf,
    h_buf,
    acc_buf,
    r_buf,
    load_sem,
    l_ssem,
    l_rsem,
    c_ssem,
    c_rsem,
    f_ssem,
    f_rsem,
    m_ssem,
    m_rsem,
    w_ssem,
    w_rsem,
    y_ssem,
    y_rsem,
    x_ssem,
    x_rsem,
    a_ssem,
    a_rsem,
    s_ssem,
    s_rsem,
):
    sp, tp = sizes
    s = lax.axis_index("sp")
    t = lax.axis_index("tp")
    core = t % 2
    x = t // 2
    y = s % 2
    zl = (s // 2) % 2
    zh = s // 4
    other = t + 1 - 2 * core
    rows = latent_ref.shape[0]
    part = rows // tp
    hid, cols = down_hbm.shape[1:]
    kv_width = latent_ref.shape[1]
    lanes = cols // 2
    quarter = sp // 2 * lanes
    width = ow_hbm.shape[1]
    along_x = (s, (1 - x) * 2 + core)

    def ring(q):
        flip = lambda bit, by: bit + by * (1 - 2 * bit)
        return flip(zh, q // 4) * 4 + flip(zl, q // 2 % 2) * 2 + flip(y, q % 2)

    def remote(src, dst, ssem, rsem, dev):
        return pltpu.make_async_remote_copy(
            src_ref=src, dst_ref=dst, send_sem=ssem, recv_sem=rsem, device_id=dev, device_id_type=MESH
        )

    def send(src, dst, ssem, rsem, dev):
        remote(src, dst, ssem, rsem, dev).start()

    def sent(ref, ssem):
        remote(ref, ref, ssem, ssem, (s, other)).wait_send()

    def arrived(ref, rsem):
        remote(ref, ref, rsem, rsem, (s, other)).wait_recv()

    barrier = pltpu.get_barrier_semaphore()
    for q in range(1, sp):
        pl.semaphore_signal(barrier, inc=1, device_id=(ring(q), t), device_id_type=MESH)
    for j in range(1, tp):
        pl.semaphore_signal(barrier, inc=1, device_id=(s, (t + j) % tp), device_id_type=MESH)

    own_rows = pl.ds(pl.multiple_of(t * part, part), part)
    own_cols = pl.ds(pl.multiple_of(s * cols, cols), cols)
    own_lanes = pl.ds(pl.multiple_of(s * lanes, lanes), lanes)
    loads = [
        pltpu.make_async_copy(src, dst, load_sem.at[i])
        for i, (src, dst) in enumerate(
            [
                (gate_hbm, raw_buf.at[0]),
                (up_hbm, raw_buf.at[1]),
                (kup_hbm, kup_ref),
                (vup_hbm, vup_ref),
                (turn_hbm, turn_ref),
                (query_hbm, query_ref),
                (ow_hbm, ow_ref),
                (resid_hbm.at[own_rows], resid_ref),
                (down_hbm.at[s, :, :lanes], wd_buf.at[0, core, :, own_lanes]),
                (down_hbm.at[s, :, lanes:], wd_buf.at[1, core, :, own_lanes]),
                (down_hbm, wt_buf.at[2]),
            ]
        )
    ]
    for load in loads:
        load.start()

    position = (s * rows + lax.broadcasted_iota(jnp.int32, (rows, 128), 0)).astype(F32)
    angles = position * inv_ref[...]
    sign = jnp.where(lax.broadcasted_iota(jnp.int32, (rows, 128), 1) % ROPE < ROPE // 2, -1.0, 1.0)
    cosine = jnp.cos(angles)
    sine = jnp.sin(angles) * sign
    lat = latent_ref[...].astype(F32)
    lat = lat * lax.rsqrt(jnp.mean(lat * lat, axis=-1, keepdims=True) + 1e-06) * lgain_ref[...]
    own_lat = lat.astype(BF)
    shared = shared_ref[...].astype(F32)
    shared = jnp.concatenate([shared] * (128 // ROPE), axis=0).T
    own_key = turn(shared, cosine, sine).astype(BF)
    for j in range(tp):
        part_of = slice(j * part, (j + 1) * part)
        kv_buf[0, j, :, :kv_width] = own_lat[part_of]
        kv_buf[0, j, :, kv_width:] = own_key[part_of]

    pl.semaphore_wait(barrier, sp - 1 + tp - 1)

    along_y = (ring(1), t)

    def send_latent(slot, by):
        to = slot + by
        send(kv_buf.at[slot, t], kv_buf.at[to, t], l_ssem.at[0], l_rsem.at[to], (ring(by), t))

    for by in (6, 4, 2, 1):
        send_latent(0, by)

    for which in range(2):
        loads[which].wait()
        turned_buf = wt_buf.at[which].reshape(sp * hid, cols)
        for j in range(raw_buf.shape[2] // 128):
            tile = slice(j * 128, (j + 1) * 128)
            turned_buf[tile, :] = raw_buf[which, :, tile].T

    first = (
        [(0, 2), (0, 6), (1, 2), (1, 6), (0, 4)],
        [(0, 2), (1, 2), (0, 6), (1, 6), (0, 4), (1, 4)],
    )
    between = ([], [(0, 7)])
    second = ([], [(1, 7)])
    third = (
        [(1, 4), (0, 3), (0, 7), (1, 3), (1, 7), (0, 5), (1, 5)],
        [(0, 3), (1, 3), (0, 5), (1, 5)],
    )
    fourth = [(w, q) for w in (2, 3) for q in (2, 3, 6, 7, 4, 5)]
    outer = zl == zh

    def late(which, q):
        return int(q in (7, 5, 3) if which < 2 else q > 3)

    def weight_slot(which, lane_of, side=core):
        if which < 2:
            return w_buf.at[which, side, :, pl.ds(pl.multiple_of(lane_of * cols, cols), cols)]
        return wd_buf.at[which - 2, side, :, pl.ds(pl.multiple_of(lane_of * lanes, lanes), lanes)]

    def lanes_of(ref, which):
        return ref if which < 2 else ref.at[:, (which - 2) * lanes:(which - 1) * lanes]

    def send_weights(some):
        for which, q in some:
            kind = min(which, 2)
            if q > 1 and q % 2:
                src, owner, dest = relay_buf.at[kind, q // 2 - 1], ring(1), (ring(q - 1), t)
            else:
                src, owner, dest = wt_buf.at[kind, ring(q)], s, (ring(q), t)
            send(
                lanes_of(src, which),
                weight_slot(which, owner),
                w_ssem.at[which],
                w_rsem.at[which, late(which, q)],
                dest,
            )

    def send_relays(kind):
        for q in (7, 5, 3):
            send(
                wt_buf.at[kind, ring(q)], relay_buf.at[kind, q // 2 - 1], y_ssem.at[kind], y_rsem.at[kind], along_y
            )
        send_weights([(which, 1) for which in ((kind,) if kind < 2 else (2, 3))])

    def relayed(kind):
        arrived(relay_buf.at[kind], y_rsem.at[kind])

    def send_by_place(lists):
        @pl.when(outer)
        def _():
            send_weights(lists[0])

        @pl.when(jnp.logical_not(outer))
        def _():
            send_weights(lists[1])

    def some_of(which, side, count):
        if which < 2:
            return w_buf.at[which, side, :, :count * cols]
        return wd_buf.at[which - 2, side, :, :count * lanes]

    def pass_weights(which, group):
        some = [q for q in range(1, sp) if late(which, q) == group]
        arrived(some_of(which, core, len(some)), w_rsem.at[which, group])
        for q in [0] * (1 - group) + some:
            slot = weight_slot(which, ring(q))
            send(slot, slot, x_ssem.at[which], x_rsem.at[which], (s, other))

    def passed_weights(which):
        arrived(some_of(which, 1 - core, sp), x_rsem.at[which])

    send_relays(0)
    send_relays(1)
    for which in range(2):
        w_buf[which, core, :, own_cols] = wt_buf[which, s]

    def make_kv(k):
        piece = kv_buf[k].reshape(rows, kv_buf.shape[3])
        piece_lat = piece[:, :kv_width]
        key_buf[k * rows:(k + 1) * rows, :] = jnp.dot(
            piece_lat, kup_ref[...], preferred_element_type=F32
        ).astype(BF)
        val_buf[k * rows:(k + 1) * rows, :] = jnp.dot(
            piece_lat, vup_ref[...], preferred_element_type=F32
        ).astype(BF)

    for load in loads[2:10]:
        load.wait()
    make_kv(0)
    query_rot = turn(
        turn_ref[...].astype(F32),
        jnp.concatenate([cosine] * (turn_ref.shape[1] // 128), axis=1),
        jnp.concatenate([sine] * (turn_ref.shape[1] // 128), axis=1),
    ).astype(BF)

    def pass_latent(slot, quarter):
        piece = kv_buf.at[slot, quarter]
        send(piece, piece, f_ssem.at[0], f_rsem.at[slot], (s, other))

    def take_latent(slot):
        piece = kv_buf.at[slot, t]
        arrived(piece, l_rsem.at[slot])
        send(piece, piece, c_ssem.at[0], c_rsem.at[slot], along_x)
        pass_latent(slot, t)

    take_latent(1)
    for by in (6, 4, 2):
        send_latent(1, by)
    loads[10].wait()
    send_relays(2)
    order = (2, 4, 6, 3, 5, 7)
    for slot in order:
        take_latent(slot)
    send_by_place(first)
    for slot in (1,) + order:
        arrived(kv_buf.at[slot, along_x[1]], c_rsem.at[slot])
        pass_latent(slot, along_x[1])
    for slot in (1,) + order:
        arrived(kv_buf.at[slot, pl.ds(0, tp // 2)], f_rsem.at[slot])
        make_kv(slot)

    scale = (NOPE + ROPE) ** (-0.5)
    all_rot = kv_buf[...].reshape(sp * rows, kv_buf.shape[3])[:, kv_width:]
    lane = lax.broadcasted_iota(jnp.int32, (rows, 128), 1)
    for pair in range(query_ref.shape[1] // 128):
        span = slice(pair * 128, (pair + 1) * 128)
        keys = jnp.concatenate([key_buf[:, span], all_rot], axis=1)
        vals = val_buf[:, span]
        results = []
        for inner in range(2):
            head = pair * 2 + inner
            tile = head * ROPE // 128
            group = head % (128 // ROPE)
            q_plain = jnp.where(lane // NOPE == inner, query_ref[:, span], jnp.zeros((), BF))
            q_turn = jnp.where(
                lane // ROPE == group, query_rot[:, tile * 128:(tile + 1) * 128], jnp.zeros((), BF)
            )
            score = lax.dot_general(
                jnp.concatenate([q_plain, q_turn], axis=1), keys, BY_LAST, preferred_element_type=F32
            ) * scale
            top = jnp.max(score, axis=-1, keepdims=True)
            expo = jnp.exp(score - top)
            total = jnp.sum(expo, axis=-1, keepdims=True)
            results.append(jnp.dot(expo.astype(BF), vals, preferred_element_type=F32) / total)
        att_buf[:, span] = jnp.where(lane < V, results[0], results[1]).astype(BF)

    relayed(0)
    send_by_place(between)
    span_of = [slice(c * width // 2, (c + 1) * width // 2) for c in range(2)]
    for c, span in enumerate(span_of):
        mix = jnp.dot(att_buf[...], ow_ref[:, span], preferred_element_type=F32)
        mix_buf[:, span] = mix
        for dest in range(tp):
            pair_buf[dest % 2, c, dest // 2] = mix[dest * part:(dest + 1) * part].astype(BF)
        send(pair_buf.at[1 - core, c], paird_buf.at[c], m_ssem.at[c], m_rsem.at[c], (s, other))
    cross_rows = pl.ds(pl.multiple_of(((1 - x) * 2 + core) * part, part), part)
    for c, span in enumerate(span_of):
        arrived(paird_buf.at[c], m_rsem.at[c])
        cross_buf[c] = (mix_buf[cross_rows, span] + paird_buf[c, 1 - x].astype(F32)).astype(BF)
        send(cross_buf.at[c], crossr_buf.at[c], m_ssem.at[2 + c], m_rsem.at[2 + c], along_x)
    mids = [
        resid_ref[:, span].astype(F32) + mix_buf[own_rows, span] + paird_buf[c, x].astype(F32)
        for c, span in enumerate(span_of)
    ]
    for c in range(2):
        arrived(crossr_buf.at[c], m_rsem.at[2 + c])
        mids[c] = mids[c] + crossr_buf[c].astype(F32)
    mid = jnp.concatenate(mids, axis=1)
    mid_buf[...] = mid
    normed = mid * lax.rsqrt(jnp.mean(mid * mid, axis=-1, keepdims=True) + 1e-06) * mgain_ref[...]
    n_buf[0] = normed.astype(BF)

    a_x = 1 - core
    pick = lambda first_x, i: first_x * along_x[i] + (1 - first_x) * along_y[i]
    steps = (
        (8, (pick(a_x, 0), pick(a_x, 1))),
        (4, (pick(core, 0), pick(core, 1))),
        (2, (ring(2), t)),
        (1, (ring(4), t)),
    )

    def spread(slot):
        for by, dev in reversed(steps):
            if by > slot:
                to = slot + by
                send(n_buf.at[slot], n_buf.at[to], a_ssem.at[0], a_rsem.at[min(to, sp)], dev)

    spread(0)
    relayed(1)
    send_by_place(second)
    arrived(n_buf.at[1], a_rsem.at[1])
    spread(1)
    send_by_place(third)
    relayed(2)
    send_weights(fourth)
    for slot in (2, 3):
        arrived(n_buf.at[slot], a_rsem.at[slot])
        spread(slot)
    for slot in (4, 5, 6, 7):
        arrived(n_buf.at[slot], a_rsem.at[slot])
        spread(slot)
    pass_weights(0, 0)
    pass_weights(1, 0)
    pass_weights(0, 1)
    pass_weights(1, 1)
    group = n_buf.shape[0] // 2

    def hidden_of(side):
        for g in range(2):
            block = n_buf[g * group:(g + 1) * group].reshape(group * part, width)
            gate = lax.dot_general(block, w_buf[0, side], BY_LAST, preferred_element_type=F32)
            up = lax.dot_general(block, w_buf[1, side], BY_LAST, preferred_element_type=F32)
            hidden = (gate / (1.0 + jnp.exp(-gate)) * up).astype(BF)
            for k in range(group):
                slot = k % 2 * 8 + g * 4 + k // 2 % 2 * 2 + k // 4
                h_buf[side, slot * part:(slot + 1) * part, :] = hidden[k * part:(k + 1) * part]

    arrived(n_buf.at[pl.ds(group, group)], a_rsem.at[sp])
    hidden_of(core)
    passed_weights(0)
    passed_weights(1)
    hidden_of(1 - core)

    to_first, to_second, to_low, to_high = (dev for by, dev in steps)
    messages = {
        14: (2, to_first),
        12: (2, to_first),
        10: (2, to_low),
        9: (1, to_second),
        8: (1, to_high),
        6: (2, to_first),
        4: (2, to_first),
        2: (2, to_low),
        1: (1, to_second),
    }
    index_of = {slot: i for i, slot in enumerate(messages)}

    def sums(q, slot):
        count, dev = messages[slot]
        some = pl.ds(slot, count)
        send(acc_buf.at[q, some], r_buf.at[q, some], s_ssem.at[q], s_rsem.at[q, index_of[slot]], dev)

    def project(h):
        for g in (1, 0):
            span = slice(g * group * part, (g + 1) * group * part)
            down = jnp.dot(h_buf[0, span], wd_buf[h, 0], preferred_element_type=F32) + jnp.dot(
                h_buf[1, span], wd_buf[h, 1], preferred_element_type=F32
            )
            for c in range(2):
                acc_buf[2 * h + c, g * group:(g + 1) * group] = (
                    down[:, c * quarter:(c + 1) * quarter].astype(BF).reshape(group, part, quarter)
                )
            for c in range(2):
                sums(2 * h + c, g * group + 6)
                sums(2 * h + c, g * group + 4)

    def landed(q, slot):
        count = messages[slot][0]
        arrived(r_buf.at[q, pl.ds(slot, count)], s_rsem.at[q, index_of[slot]])
        return r_buf[q, slot:slot + count].astype(F32)

    def join(q, to, *slots):
        count = messages[slots[0]][0]
        value = acc_buf[q, to:to + count].astype(F32)
        for slot in slots:
            value = value + landed(q, slot)
        acc_buf[q, to:to + count] = value.astype(BF)

    def to_10(q):
        join(q, 10, 14)
        sums(q, 10)

    def to_2(q):
        join(q, 2, 6)
        sums(q, 2)

    def to_9(q):
        join(q, 8, 12, 10)
        sums(q, 9)

    def to_8(q):
        join(q, 8, 9)
        sums(q, 8)

    def to_1(q):
        join(q, 0, 4, 2)
        sums(q, 1)

    def finish(q):
        value = acc_buf[q, 0].astype(F32) + landed(q, 1)[0] + landed(q, 8)[0]
        h, c = q // 2, q % 2
        for k in range(sp // 2):
            start = (c * sp // 2 + k) * cols + h * lanes
            span = slice(start, start + lanes)
            out_ref[:, span] = (
                mid_buf[:, span] + 0.5 * value[:, k * lanes:(k + 1) * lanes]
            ).astype(BF)

    pass_weights(2, 0)
    pass_weights(2, 1)
    passed_weights(2)
    project(0)
    to_10(0)
    to_10(1)
    to_2(0)
    pass_weights(3, 0)
    pass_weights(3, 1)
    to_2(1)
    to_9(0)
    to_9(1)
    passed_weights(3)
    project(1)
    to_8(0)
    to_8(1)
    to_10(2)
    to_10(3)
    to_1(0)
    to_1(1)
    to_2(2)
    finish(0)
    to_9(2)
    to_2(3)
    finish(1)
    to_9(3)
    to_8(2)
    to_1(2)
    to_8(3)
    to_1(3)
    finish(2)
    finish(3)

    for h in range(4):
        sent(r_buf.at[h, pl.ds(1, 2 * sp - 1)], s_ssem.at[h])
    sent(n_buf.at[pl.ds(1, 2 * sp - 1)], a_ssem.at[0])
    for c in range(2):
        sent(paird_buf.at[c], m_ssem.at[c])
        sent(crossr_buf.at[c], m_ssem.at[2 + c])
    sent(kv_buf.at[pl.ds(1, sp - 1), 0], l_ssem.at[0])
    sent(kv_buf.at[pl.ds(1, sp - 1), 0], c_ssem.at[0])
    sent(kv_buf.at[pl.ds(1, sp - 1), pl.ds(0, tp // 2)], f_ssem.at[0])
    for kind in range(3):
        sent(relay_buf.at[kind], y_ssem.at[kind])
    for which in range(4):
        sent(some_of(which, core, sp - 1), w_ssem.at[which])
        sent(some_of(which, core, sp), x_ssem.at[which])


def fused_layer(
    resid_in,
    query_plain,
    query_turn,
    latent_raw,
    shared_key,
    latent_gain,
    key_up,
    value_up,
    out_weight,
    mixer_gain,
    gate_weight,
    up_weight,
    down_weight,
):
    sp = lax.axis_size("sp")
    tp = lax.axis_size("tp")
    rows, width = resid_in.shape
    part = rows // tp
    hid = down_weight.shape[0] // sp
    cols = down_weight.shape[1]
    kv = latent_raw.shape[1]
    heads_width = query_plain.shape[1]
    inverse = 10000.0 ** (-jnp.arange(0, ROPE, 2, dtype=F32) / ROPE)
    inverse_lanes = jnp.tile(inverse, 128 * 2 // ROPE)[None, :]
    chips = sp * tp // 2
    dma = pltpu.SemaphoreType.DMA
    vmem = lambda *shape: pltpu.VMEM(shape, BF)
    near = pl.BlockSpec(memory_space=pltpu.VMEM)
    far = pl.BlockSpec(memory_space=pl.ANY)
    return pl.pallas_call(
        functools.partial(layer_kernel, (sp, tp)),
        out_shape=jax.ShapeDtypeStruct((part, width), BF),
        in_specs=[near] * 5 + [far] * 9,
        out_specs=near,
        scratch_shapes=[
            vmem(*query_plain.shape),
            vmem(*query_turn.shape),
            vmem(*key_up.shape),
            vmem(*value_up.shape),
            vmem(*out_weight.shape),
            vmem(part, width),
            vmem(2, *gate_weight.shape),
            vmem(3, sp, hid, cols),
            vmem(3, sp // 2 - 1, hid, cols),
            vmem(sp, tp, part, kv + 128),
            vmem(sp * rows, heads_width),
            vmem(sp * rows, heads_width),
            vmem(rows, heads_width),
            pltpu.VMEM((rows, width), F32),
            vmem(2, 2, tp // 2, part, width // 2),
            vmem(2, tp // 2, part, width // 2),
            vmem(2, part, width // 2),
            vmem(2, part, width // 2),
            pltpu.VMEM((part, width), F32),
            vmem(2, 2, hid, width),
            vmem(2, 2, hid, width // 2),
            vmem(chips, part, width),
            vmem(2, chips * part, hid),
            vmem(4, chips, part, width // 4),
            vmem(4, chips, part, width // 4),
            dma((11,)),
            dma((1,)),
            dma((sp,)),
            dma((1,)),
            dma((sp,)),
            dma((1,)),
            dma((sp,)),
            dma((4,)),
            dma((4,)),
            dma((4,)),
            dma((4, 2)),
            dma((3,)),
            dma((3,)),
            dma((4,)),
            dma((4,)),
            dma((1,)),
            dma((sp + 1,)),
            dma((4,)),
            dma((4, sp + 1)),
        ],
        compiler_params=pltpu.CompilerParams(
            collective_id=0, has_side_effects=True, vmem_limit_bytes=60 * 1024 * 1024
        ),
    )(
        latent_raw,
        shared_key.T,
        inverse_lanes,
        latent_gain[None, :],
        mixer_gain[None, :],
        query_plain,
        query_turn,
        key_up,
        value_up,
        out_weight,
        resid_in,
        gate_weight,
        up_weight,
        down_weight.reshape(sp, hid, cols),
    )


def per_device(*arrays):
    resid_in, query_plain, query_turn, latent_raw = arrays[:4]
    down_weight = arrays[-1]
    sp = lax.axis_size("sp")
    tp = lax.axis_size("tp")
    rows = resid_in.shape[0]
    fits = (
        sp // 4 == 2
        and tp // 2 == 2
        and rows % (32 * tp) == 0
        and down_weight.shape[0] % (16 * sp) == 0
        and down_weight.shape[1] % 128 == 0
        and latent_raw.shape[1] % 128 == 0
        and query_plain.shape[1] % 128 == 0
        and query_turn.shape[1] % 128 == 0
        and rows * sp <= 1024
        and sp * tp <= 32
    )
    if fits:
        return fused_layer(*arrays)
    return plain_layer(*arrays)


def solution(mesh):
    return jax.shard_map(
        per_device,
        mesh=mesh,
        in_specs=(
            P("sp", None),
            P("sp", "tp"),
            P("sp", "tp"),
            P("sp", None),
            P("sp", None),
            P(),
            P(None, "tp"),
            P(None, "tp"),
            P("tp", None),
            P(),
            P("sp", "tp"),
            P("sp", "tp"),
            P("tp", "sp"),
        ),
        out_specs=P(("sp", "tp"), None),
        check_vma=False,
    )
```

```python
import functools
import math

import jax
import jax.numpy as jnp
from jax import lax
from jax.experimental import pallas as pl
from jax.experimental.pallas import tpu as pltpu
from jax.sharding import PartitionSpec as P

NOPE = 64
ROPE = 32
V = 64


def rotate(values, cosine, sine):
    half_width = values.shape[-1] // 2
    first = values[..., :half_width]
    second = values[..., half_width:]
    return jnp.concatenate(
        [first * cosine - second * sine, first * sine + second * cosine], axis=-1
    )


def rms_scale(values, gain):
    return values * lax.rsqrt(jnp.mean(values * values, axis=-1, keepdims=True) + 1e-06) * gain


def plain_layer(
    resid_in,
    query_plain,
    query_turn,
    latent_raw,
    shared_key,
    latent_gain,
    key_up,
    value_up,
    out_weight,
    mixer_gain,
    gate_weight,
    up_weight,
    down_weight,
):
    tok_rows = resid_in.shape[0]
    head_count = query_plain.shape[1] // NOPE
    part_rows = tok_rows // lax.axis_size("tp")
    offset = lax.axis_index("sp") * tok_rows
    position = (offset + jnp.arange(tok_rows, dtype=jnp.int32)).astype(jnp.float32)
    inverse = 10000.0 ** (-jnp.arange(0, ROPE, 2, dtype=jnp.float32) / ROPE)
    angles = position[:, None] * inverse[None, :]
    cosine = jnp.cos(angles)
    sine = jnp.sin(angles)
    query_heads = query_plain.reshape(tok_rows, head_count, NOPE)
    query_rot = rotate(
        query_turn.reshape(tok_rows, head_count, ROPE).astype(jnp.float32),
        cosine[:, None, :],
        sine[:, None, :],
    ).astype(jnp.bfloat16)
    latent = rms_scale(latent_raw.astype(jnp.float32), latent_gain).astype(jnp.bfloat16)
    key_rot = rotate(shared_key.astype(jnp.float32), cosine, sine).astype(jnp.bfloat16)
    softmax_scale = (NOPE + ROPE) ** (-0.5)

    def attend_block(state, key_plain, values, key_pos):
        run_max, run_total, run_acc = state
        score = jnp.einsum(
            "qhd,khd->hqk", query_heads, key_plain, preferred_element_type=jnp.float32
        )
        score = score + jnp.einsum(
            "qhr,kr->hqk", query_rot, key_pos, preferred_element_type=jnp.float32
        )
        score = score * softmax_scale
        new_max = jnp.maximum(run_max, jnp.max(score, axis=-1))
        shrink = jnp.exp(run_max - new_max)
        expo = jnp.exp(score - new_max[:, :, None])
        run_total = run_total * shrink + jnp.sum(expo, axis=-1)
        run_acc = run_acc * shrink.T[:, :, None] + jnp.einsum(
            "hqk,khd->qhd", expo.astype(jnp.bfloat16), values, preferred_element_type=jnp.float32
        )
        return (new_max, run_total, run_acc)

    start_state = (
        jnp.full((head_count, tok_rows), -jnp.inf, jnp.float32),
        jnp.zeros((head_count, tok_rows), jnp.float32),
        jnp.zeros((tok_rows, head_count, V), jnp.float32),
    )
    state = start_state
    latent_piece = lax.all_gather(latent, "sp", axis=0, tiled=True)
    pos_piece = lax.all_gather(key_rot, "sp", axis=0, tiled=True)
    piece_len = latent_piece.shape[0]
    block_len = math.gcd(piece_len, 512)
    block_count = piece_len // block_len

    def one_block(inner, items):
        latent_rows, pos_rows = items
        key_plain = (
            jnp.dot(latent_rows, key_up, preferred_element_type=jnp.float32)
            .astype(jnp.bfloat16)
            .reshape(block_len, head_count, NOPE)
        )
        values = (
            jnp.dot(latent_rows, value_up, preferred_element_type=jnp.float32)
            .astype(jnp.bfloat16)
            .reshape(block_len, head_count, V)
        )
        return (attend_block(inner, key_plain, values, pos_rows), None)

    state, unused = lax.scan(
        one_block,
        state,
        (
            latent_piece.reshape(block_count, block_len, latent_piece.shape[1]),
            pos_piece.reshape(block_count, block_len, ROPE),
        ),
    )
    attended = (
        (state[2] / state[1].T[:, :, None]).astype(jnp.bfloat16).reshape(tok_rows, head_count * V)
    )
    own_start = lax.axis_index("tp") * part_rows
    mixed = lax.psum_scatter(
        jnp.dot(attended, out_weight, preferred_element_type=jnp.float32).astype(jnp.bfloat16),
        "tp",
        scatter_dimension=0,
        tiled=True,
    ).astype(jnp.float32)
    middle = lax.dynamic_slice_in_dim(resid_in, own_start, part_rows, 0).astype(jnp.float32) + mixed
    normed = rms_scale(middle, mixer_gain).astype(jnp.bfloat16)
    all_rows = lax.all_gather(normed, "tp", axis=0, tiled=True)
    gate_sum = jnp.dot(
        all_rows,
        lax.all_gather(gate_weight, "sp", axis=0, tiled=True),
        preferred_element_type=jnp.float32,
    )
    up_sum = jnp.dot(
        all_rows,
        lax.all_gather(up_weight, "sp", axis=0, tiled=True),
        preferred_element_type=jnp.float32,
    )
    hidden = (jax.nn.silu(gate_sum) * up_sum).astype(jnp.bfloat16)
    terms = jnp.dot(
        hidden,
        lax.all_gather(down_weight, "sp", axis=1, tiled=True),
        preferred_element_type=jnp.float32,
    )
    down_sum = lax.psum_scatter(
        terms.astype(jnp.bfloat16), "tp", scatter_dimension=0, tiled=True
    ).astype(jnp.float32)
    return (middle + 0.5 * down_sum).astype(jnp.bfloat16)

MESH = pl.DeviceIdType.MESH
BF = jnp.bfloat16
F32 = jnp.float32
BY_LAST = (((1,), (1,)), ((), ()))


def turn(values, cosine, sine):
    width = values.shape[-1]
    half = ROPE // 2
    lane = lax.broadcasted_iota(jnp.int32, values.shape, 1) % ROPE
    swapped = jnp.where(lane < half, pltpu.roll(values, width - half, 1), pltpu.roll(values, half, 1))
    return values * cosine + swapped * sine


def layer_kernel(
    sizes,
    latent_ref,
    shared_ref,
    inv_ref,
    lgain_ref,
    mgain_ref,
    query_hbm,
    turn_hbm,
    kup_hbm,
    vup_hbm,
    ow_hbm,
    resid_hbm,
    gate_hbm,
    up_hbm,
    down_hbm,
    out_ref,
    query_ref,
    turn_ref,
    kup_ref,
    vup_ref,
    ow_ref,
    resid_ref,
    raw_buf,
    wt_buf,
    relay_buf,
    kv_buf,
    key_buf,
    val_buf,
    att_buf,
    mix_buf,
    pair_buf,
    paird_buf,
    cross_buf,
    crossr_buf,
    mid_buf,
    w_buf,
    wd_buf,
    n_buf,
    h_buf,
    acc_buf,
    r_buf,
    load_sem,
    l_ssem,
    l_rsem,
    c_ssem,
    c_rsem,
    f_ssem,
    f_rsem,
    m_ssem,
    m_rsem,
    w_ssem,
    w_rsem,
    y_ssem,
    y_rsem,
    x_ssem,
    x_rsem,
    a_ssem,
    a_rsem,
    s_ssem,
    s_rsem,
):
    sp, tp = sizes
    s = lax.axis_index("sp")
    t = lax.axis_index("tp")
    core = t % 2
    x = t // 2
    y = s % 2
    zl = (s // 2) % 2
    zh = s // 4
    other = t + 1 - 2 * core
    rows = latent_ref.shape[0]
    part = rows // tp
    hid, cols = down_hbm.shape[1:]
    kv_width = latent_ref.shape[1]
    lanes = cols // 2
    quarter = sp // 2 * lanes
    width = ow_hbm.shape[1]
    along_x = (s, (1 - x) * 2 + core)

    def ring(q):
        flip = lambda bit, by: bit + by * (1 - 2 * bit)
        return flip(zh, q // 4) * 4 + flip(zl, q // 2 % 2) * 2 + flip(y, q % 2)

    def remote(src, dst, ssem, rsem, dev):
        return pltpu.make_async_remote_copy(
            src_ref=src, dst_ref=dst, send_sem=ssem, recv_sem=rsem, device_id=dev, device_id_type=MESH
        )

    def send(src, dst, ssem, rsem, dev):
        remote(src, dst, ssem, rsem, dev).start()

    def sent(ref, ssem):
        remote(ref, ref, ssem, ssem, (s, other)).wait_send()

    def arrived(ref, rsem):
        remote(ref, ref, rsem, rsem, (s, other)).wait_recv()

    barrier = pltpu.get_barrier_semaphore()
    for q in range(1, sp):
        pl.semaphore_signal(barrier, inc=1, device_id=(ring(q), t), device_id_type=MESH)
    for j in range(1, tp):
        pl.semaphore_signal(barrier, inc=1, device_id=(s, (t + j) % tp), device_id_type=MESH)
    for q in (2, 4):
        pl.semaphore_signal(barrier, inc=1, device_id=(ring(q), along_x[1]), device_id_type=MESH)

    own_rows = pl.ds(pl.multiple_of(t * part, part), part)
    own_cols = pl.ds(pl.multiple_of(s * cols, cols), cols)
    own_lanes = pl.ds(pl.multiple_of(s * lanes, lanes), lanes)
    loads = [
        pltpu.make_async_copy(src, dst, load_sem.at[i])
        for i, (src, dst) in enumerate(
            [
                (gate_hbm, raw_buf.at[0]),
                (up_hbm, raw_buf.at[1]),
                (kup_hbm, kup_ref),
                (vup_hbm, vup_ref),
                (turn_hbm, turn_ref),
                (query_hbm, query_ref),
                (ow_hbm, ow_ref),
                (resid_hbm.at[own_rows], resid_ref),
                (down_hbm.at[s, :, :lanes], wd_buf.at[0, core, :, own_lanes]),
                (down_hbm.at[s, :, lanes:], wd_buf.at[1, core, :, own_lanes]),
                (down_hbm, wt_buf.at[2]),
            ]
        )
    ]
    for load in loads:
        load.start()

    position = (s * rows + lax.broadcasted_iota(jnp.int32, (rows, 128), 0)).astype(F32)
    angles = position * inv_ref[...]
    sign = jnp.where(lax.broadcasted_iota(jnp.int32, (rows, 128), 1) % ROPE < ROPE // 2, -1.0, 1.0)
    cosine = jnp.cos(angles)
    sine = jnp.sin(angles) * sign
    lat = latent_ref[...].astype(F32)
    lat = lat * lax.rsqrt(jnp.mean(lat * lat, axis=-1, keepdims=True) + 1e-06) * lgain_ref[...]
    own_lat = lat.astype(BF)
    shared = shared_ref[...].astype(F32)
    shared = jnp.concatenate([shared] * (128 // ROPE), axis=0).T
    own_key = turn(shared, cosine, sine).astype(BF)
    for j in range(tp):
        part_of = slice(j * part, (j + 1) * part)
        kv_buf[0, j, :, :kv_width] = own_lat[part_of]
        kv_buf[0, j, :, kv_width:] = own_key[part_of]

    pl.semaphore_wait(barrier, sp - 1 + tp + 1)

    along_y = (ring(1), t)

    def send_latent(slot, by):
        to = slot + by
        send(kv_buf.at[slot, t], kv_buf.at[to, t], l_ssem.at[0], l_rsem.at[to], (ring(by), t))

    for by in (6, 4, 2, 1):
        send_latent(0, by)

    for which in range(2):
        loads[which].wait()
        turned_buf = wt_buf.at[which].reshape(sp * hid, cols)
        for j in range(raw_buf.shape[2] // 128):
            tile = slice(j * 128, (j + 1) * 128)
            turned_buf[tile, :] = raw_buf[which, :, tile].T

    first = (
        [(0, 2), (0, 6), (1, 2), (1, 6), (0, 4)],
        [(0, 2), (1, 2), (0, 6), (1, 6), (0, 4), (1, 4)],
    )
    between = ([], [(0, 7)])
    second = ([], [(1, 7)])
    third = (
        [(1, 4), (0, 3), (0, 7), (1, 3), (1, 7), (0, 5), (1, 5)],
        [(0, 3), (1, 3), (0, 5), (1, 5)],
    )
    fourth = [(w, q) for w in (2, 3) for q in (2, 3, 6, 7, 4, 5)]
    outer = zl == zh

    def late(which, q):
        return int(q in (7, 5, 3) if which < 2 else q > 3)

    def weight_slot(which, lane_of, side=core):
        if which < 2:
            return w_buf.at[which, side, :, pl.ds(pl.multiple_of(lane_of * cols, cols), cols)]
        return wd_buf.at[which - 2, side, :, pl.ds(pl.multiple_of(lane_of * lanes, lanes), lanes)]

    def lanes_of(ref, which):
        return ref if which < 2 else ref.at[:, (which - 2) * lanes:(which - 1) * lanes]

    def send_weights(some):
        for which, q in some:
            kind = min(which, 2)
            if q > 1 and q % 2:
                src, owner, dest = relay_buf.at[kind, q // 2 - 1], ring(1), (ring(q - 1), t)
            else:
                src, owner, dest = wt_buf.at[kind, ring(q)], s, (ring(q), t)
            send(
                lanes_of(src, which),
                weight_slot(which, owner),
                w_ssem.at[which],
                w_rsem.at[which, late(which, q)],
                dest,
            )

    def send_relays(kind):
        for q in (7, 5, 3):
            send(
                wt_buf.at[kind, ring(q)], relay_buf.at[kind, q // 2 - 1], y_ssem.at[kind], y_rsem.at[kind], along_y
            )
        send_weights([(which, 1) for which in ((kind,) if kind < 2 else (2, 3))])

    def relayed(kind):
        arrived(relay_buf.at[kind], y_rsem.at[kind])

    def send_by_place(lists):
        @pl.when(outer)
        def _():
            send_weights(lists[0])

        @pl.when(jnp.logical_not(outer))
        def _():
            send_weights(lists[1])

    def some_of(which, side, count):
        if which < 2:
            return w_buf.at[which, side, :, :count * cols]
        return wd_buf.at[which - 2, side, :, :count * lanes]

    def pass_weights(which, group):
        some = [q for q in range(1, sp) if late(which, q) == group]
        arrived(some_of(which, core, len(some)), w_rsem.at[which, group])
        for q in [0] * (1 - group) + some:
            slot = weight_slot(which, ring(q))
            send(slot, slot, x_ssem.at[which], x_rsem.at[which], (s, other))

    def passed_weights(which):
        arrived(some_of(which, 1 - core, sp), x_rsem.at[which])

    send_relays(0)
    send_relays(1)
    for which in range(2):
        w_buf[which, core, :, own_cols] = wt_buf[which, s]

    def make_kv(k):
        piece = kv_buf[k].reshape(rows, kv_buf.shape[3])
        piece_lat = piece[:, :kv_width]
        key_buf[k * rows:(k + 1) * rows, :] = jnp.dot(
            piece_lat, kup_ref[...], preferred_element_type=F32
        ).astype(BF)
        val_buf[k * rows:(k + 1) * rows, :] = jnp.dot(
            piece_lat, vup_ref[...], preferred_element_type=F32
        ).astype(BF)

    for load in loads[2:10]:
        load.wait()
    make_kv(0)
    query_rot = turn(
        turn_ref[...].astype(F32),
        jnp.concatenate([cosine] * (turn_ref.shape[1] // 128), axis=1),
        jnp.concatenate([sine] * (turn_ref.shape[1] // 128), axis=1),
    ).astype(BF)

    def pass_latent(slot, quarter):
        piece = kv_buf.at[slot, quarter]
        send(piece, piece, f_ssem.at[0], f_rsem.at[slot], (s, other))

    def take_latent(slot):
        piece = kv_buf.at[slot, t]
        arrived(piece, l_rsem.at[slot])
        send(piece, piece, c_ssem.at[0], c_rsem.at[slot], along_x)
        pass_latent(slot, t)

    take_latent(1)
    for by in (6, 4, 2):
        send_latent(1, by)
    loads[10].wait()
    send_relays(2)
    order = (2, 4, 6, 3, 5, 7)
    for slot in order:
        take_latent(slot)
    send_by_place(first)
    def take_block(slot):
        arrived(kv_buf.at[slot, pl.ds(0, tp // 2)], f_rsem.at[slot])
        make_kv(slot)

    order = (1,) + order
    for i, slot in enumerate(order):
        arrived(kv_buf.at[slot, along_x[1]], c_rsem.at[slot])
        pass_latent(slot, along_x[1])
        if i > 1:
            take_block(order[i - 2])
    for slot in order[-2:]:
        take_block(slot)

    scale = (NOPE + ROPE) ** (-0.5) * math.log2(math.e)
    all_rot = kv_buf[...].reshape(sp * rows, kv_buf.shape[3])[:, kv_width:]
    lane = lax.broadcasted_iota(jnp.int32, (rows, 128), 1)
    for pair in range(query_ref.shape[1] // 128):
        span = slice(pair * 128, (pair + 1) * 128)
        keys = jnp.concatenate([key_buf[:, span], all_rot], axis=1)
        vals = val_buf[:, span]
        results = []
        for inner in range(2):
            head = pair * 2 + inner
            tile = head * ROPE // 128
            group = head % (128 // ROPE)
            q_plain = jnp.where(lane // NOPE == inner, query_ref[:, span], jnp.zeros((), BF))
            q_turn = jnp.where(
                lane // ROPE == group, query_rot[:, tile * 128:(tile + 1) * 128], jnp.zeros((), BF)
            )
            score = lax.dot_general(
                jnp.concatenate([q_plain, q_turn], axis=1), keys, BY_LAST, preferred_element_type=F32
            )
            top = jnp.max(score, axis=-1, keepdims=True)
            expo = jnp.exp2((score - top) * scale)
            total = jnp.sum(expo, axis=-1, keepdims=True)
            results.append(jnp.dot(expo.astype(BF), vals, preferred_element_type=F32) / total)
        att_buf[:, span] = jnp.where(lane < V, results[0], results[1]).astype(BF)

    relayed(0)
    send_by_place(between)
    span_of = [slice(c * width // 2, (c + 1) * width // 2) for c in range(2)]
    for c, span in enumerate(span_of):
        mix = jnp.dot(att_buf[...], ow_ref[:, span], preferred_element_type=F32)
        mix_buf[:, span] = mix
        for dest in range(tp):
            pair_buf[dest % 2, c, dest // 2] = mix[dest * part:(dest + 1) * part].astype(BF)
        send(pair_buf.at[1 - core, c], paird_buf.at[c], m_ssem.at[c], m_rsem.at[c], (s, other))
    cross_rows = pl.ds(pl.multiple_of(((1 - x) * 2 + core) * part, part), part)
    for c, span in enumerate(span_of):
        arrived(paird_buf.at[c], m_rsem.at[c])
        cross_buf[c] = (mix_buf[cross_rows, span] + paird_buf[c, 1 - x].astype(F32)).astype(BF)
        send(cross_buf.at[c], crossr_buf.at[c], m_ssem.at[2 + c], m_rsem.at[2 + c], along_x)
    mids = [
        resid_ref[:, span].astype(F32) + mix_buf[own_rows, span] + paird_buf[c, x].astype(F32)
        for c, span in enumerate(span_of)
    ]
    for c in range(2):
        arrived(crossr_buf.at[c], m_rsem.at[2 + c])
        mids[c] = mids[c] + crossr_buf[c].astype(F32)
    mid = jnp.concatenate(mids, axis=1)
    mid_buf[...] = mid
    normed = mid * lax.rsqrt(jnp.mean(mid * mid, axis=-1, keepdims=True) + 1e-06) * mgain_ref[...]
    n_buf[0] = normed.astype(BF)

    a_x = 1 - core
    pick = lambda first_x, i: first_x * along_x[i] + (1 - first_x) * along_y[i]
    steps = (
        (8, (pick(a_x, 0), pick(a_x, 1))),
        (4, (pick(core, 0), pick(core, 1))),
        (2, (ring(2), t)),
        (1, (ring(4), t)),
    )

    def spread(slot):
        for by, dev in reversed(steps):
            if by > slot:
                to = slot + by
                send(n_buf.at[slot], n_buf.at[to], a_ssem.at[0], a_rsem.at[min(to, sp)], dev)

    spread(0)
    relayed(1)
    send_by_place(second)
    arrived(n_buf.at[1], a_rsem.at[1])
    spread(1)
    send_by_place(third)
    relayed(2)
    send_weights(fourth)
    for slot in (2, 3):
        arrived(n_buf.at[slot], a_rsem.at[slot])
        spread(slot)
    for slot in (4, 5, 6, 7):
        arrived(n_buf.at[slot], a_rsem.at[slot])
        spread(slot)
    pass_weights(0, 0)
    pass_weights(1, 0)
    pass_weights(0, 1)
    pass_weights(1, 1)
    group = n_buf.shape[0] // 2

    def hidden_of(side):
        for g in range(2):
            block = n_buf[g * group:(g + 1) * group].reshape(group * part, width)
            gate = lax.dot_general(block, w_buf[0, side], BY_LAST, preferred_element_type=F32)
            up = lax.dot_general(block, w_buf[1, side], BY_LAST, preferred_element_type=F32)
            hidden = (gate / (1.0 + jnp.exp(-gate)) * up).astype(BF)
            for k in range(group):
                slot = k % 2 * 8 + g * 4 + k // 2 % 2 * 2 + k // 4
                h_buf[side, slot * part:(slot + 1) * part, :] = hidden[k * part:(k + 1) * part]

    arrived(n_buf.at[pl.ds(group, group)], a_rsem.at[sp])
    hidden_of(core)
    passed_weights(0)
    passed_weights(1)
    hidden_of(1 - core)

    last = (3,)
    to_first, to_second, to_low, to_high = (dev for by, dev in steps)
    messages = {
        14: (2, to_first),
        12: (2, to_first),
        10: (2, to_low),
        9: (1, to_second),
        8: (1, to_high),
        6: (2, to_first),
        4: (2, to_first),
        2: (2, to_low),
        1: (1, to_second),
    }
    index_of = {slot: i for i, slot in enumerate((*messages, 3))}

    def over(q):
        return (ring(q + 1 - core), t + core * (along_x[1] - t))

    direct = {**messages, 3: (1, over(2)), 2: (1, to_low), 9: (1, over(4))}

    def message(q, slot):
        return direct[slot] if q in last else messages[slot]

    def sums(q, slot):
        count, dev = message(q, slot)
        some = pl.ds(slot, count)
        send(acc_buf.at[q, some], r_buf.at[q, some], s_ssem.at[q], s_rsem.at[q, index_of[slot]], dev)

    def project(h):
        for g in (1, 0):
            span = slice(g * group * part, (g + 1) * group * part)
            down = jnp.dot(h_buf[0, span], wd_buf[h, 0], preferred_element_type=F32) + jnp.dot(
                h_buf[1, span], wd_buf[h, 1], preferred_element_type=F32
            )
            for c in range(2):
                acc_buf[2 * h + c, g * group:(g + 1) * group] = (
                    down[:, c * quarter:(c + 1) * quarter].astype(BF).reshape(group, part, quarter)
                )
            for c in range(2):
                sums(2 * h + c, g * group + 6)
                sums(2 * h + c, g * group + 4)

    def landed(q, slot):
        count = message(q, slot)[0]
        arrived(r_buf.at[q, pl.ds(slot, count)], s_rsem.at[q, index_of[slot]])
        return r_buf[q, slot:slot + count].astype(F32)

    def join(q, to, *slots):
        count = message(q, slots[0])[0]
        value = acc_buf[q, to:to + count].astype(F32)
        for slot in slots:
            value = value + landed(q, slot)
        acc_buf[q, to:to + count] = value.astype(BF)

    def to_10(q):
        join(q, 10, 14)
        sums(q, 10)

    def to_2(q):
        join(q, 2, 6)
        if q in last:
            sums(q, 3)
        sums(q, 2)

    def to_9(q):
        join(q, 8, 12, 10)
        sums(q, 9)
        if q in last:
            sums(q, 8)

    def to_8(q):
        if q not in last:
            join(q, 8, 9)
            sums(q, 8)

    def to_1(q):
        join(q, 0, *((4,) if q in last else (4, 2)))
        sums(q, 1)

    def finish(q):
        value = acc_buf[q, 0].astype(F32)
        for slot in (2, 3, 9, 1, 8) if q in last else (1, 8):
            value = value + landed(q, slot)[0]
        h, c = q // 2, q % 2
        for k in range(sp // 2):
            start = (c * sp // 2 + k) * cols + h * lanes
            span = slice(start, start + lanes)
            out_ref[:, span] = (
                mid_buf[:, span] + 0.5 * value[:, k * lanes:(k + 1) * lanes]
            ).astype(BF)

    pass_weights(2, 0)
    pass_weights(2, 1)
    passed_weights(2)
    project(0)
    to_10(0)
    to_10(1)
    to_2(0)
    pass_weights(3, 0)
    pass_weights(3, 1)
    to_2(1)
    to_9(0)
    to_9(1)
    passed_weights(3)
    project(1)
    to_8(0)
    to_8(1)
    to_10(2)
    to_10(3)
    to_1(0)
    to_1(1)
    to_2(2)
    to_9(2)
    to_2(3)
    finish(0)
    to_9(3)
    to_8(2)
    to_1(2)
    finish(1)
    to_1(3)
    finish(2)
    finish(3)

    for h in range(4):
        sent(r_buf.at[h, pl.ds(1, 2 * sp - 1)], s_ssem.at[h])
    sent(n_buf.at[pl.ds(1, 2 * sp - 1)], a_ssem.at[0])
    for c in range(2):
        sent(paird_buf.at[c], m_ssem.at[c])
        sent(crossr_buf.at[c], m_ssem.at[2 + c])
    sent(kv_buf.at[pl.ds(1, sp - 1), 0], l_ssem.at[0])
    sent(kv_buf.at[pl.ds(1, sp - 1), 0], c_ssem.at[0])
    sent(kv_buf.at[pl.ds(1, sp - 1), pl.ds(0, tp // 2)], f_ssem.at[0])
    for kind in range(3):
        sent(relay_buf.at[kind], y_ssem.at[kind])
    for which in range(4):
        sent(some_of(which, core, sp - 1), w_ssem.at[which])
        sent(some_of(which, core, sp), x_ssem.at[which])


def fused_layer(
    resid_in,
    query_plain,
    query_turn,
    latent_raw,
    shared_key,
    latent_gain,
    key_up,
    value_up,
    out_weight,
    mixer_gain,
    gate_weight,
    up_weight,
    down_weight,
):
    sp = lax.axis_size("sp")
    tp = lax.axis_size("tp")
    rows, width = resid_in.shape
    part = rows // tp
    hid = down_weight.shape[0] // sp
    cols = down_weight.shape[1]
    kv = latent_raw.shape[1]
    heads_width = query_plain.shape[1]
    inverse = 10000.0 ** (-jnp.arange(0, ROPE, 2, dtype=F32) / ROPE)
    inverse_lanes = jnp.tile(inverse, 128 * 2 // ROPE)[None, :]
    chips = sp * tp // 2
    dma = pltpu.SemaphoreType.DMA
    vmem = lambda *shape: pltpu.VMEM(shape, BF)
    near = pl.BlockSpec(memory_space=pltpu.VMEM)
    far = pl.BlockSpec(memory_space=pl.ANY)
    return pl.pallas_call(
        functools.partial(layer_kernel, (sp, tp)),
        out_shape=pltpu.VMEM((part, width), BF),
        in_specs=[near] * 5 + [far] * 9,
        out_specs=near,
        scratch_shapes=[
            vmem(*query_plain.shape),
            vmem(*query_turn.shape),
            vmem(*key_up.shape),
            vmem(*value_up.shape),
            vmem(*out_weight.shape),
            vmem(part, width),
            vmem(2, *gate_weight.shape),
            vmem(3, sp, hid, cols),
            vmem(3, sp // 2 - 1, hid, cols),
            vmem(sp, tp, part, kv + 128),
            vmem(sp * rows, heads_width),
            vmem(sp * rows, heads_width),
            vmem(rows, heads_width),
            pltpu.VMEM((rows, width), F32),
            vmem(2, 2, tp // 2, part, width // 2),
            vmem(2, tp // 2, part, width // 2),
            vmem(2, part, width // 2),
            vmem(2, part, width // 2),
            pltpu.VMEM((part, width), F32),
            vmem(2, 2, hid, width),
            vmem(2, 2, hid, width // 2),
            vmem(chips, part, width),
            vmem(2, chips * part, hid),
            vmem(4, chips, part, width // 4),
            vmem(4, chips, part, width // 4),
            dma((11,)),
            dma((1,)),
            dma((sp,)),
            dma((1,)),
            dma((sp,)),
            dma((1,)),
            dma((sp,)),
            dma((4,)),
            dma((4,)),
            dma((4,)),
            dma((4, 2)),
            dma((3,)),
            dma((3,)),
            dma((4,)),
            dma((4,)),
            dma((1,)),
            dma((sp + 1,)),
            dma((4,)),
            dma((4, sp + 2)),
        ],
        compiler_params=pltpu.CompilerParams(
            collective_id=0, has_side_effects=True, vmem_limit_bytes=60 * 1024 * 1024
        ),
    )(
        latent_raw,
        shared_key.T,
        inverse_lanes,
        latent_gain[None, :],
        mixer_gain[None, :],
        query_plain,
        query_turn,
        key_up,
        value_up,
        out_weight,
        resid_in,
        gate_weight,
        up_weight,
        down_weight.reshape(sp, hid, cols),
    )


def per_device(*arrays):
    resid_in, query_plain, query_turn, latent_raw = arrays[:4]
    down_weight = arrays[-1]
    sp = lax.axis_size("sp")
    tp = lax.axis_size("tp")
    rows = resid_in.shape[0]
    fits = (
        sp // 4 == 2
        and tp // 2 == 2
        and rows % (32 * tp) == 0
        and down_weight.shape[0] % (16 * sp) == 0
        and down_weight.shape[1] % 128 == 0
        and latent_raw.shape[1] % 128 == 0
        and query_plain.shape[1] % 128 == 0
        and query_turn.shape[1] % 128 == 0
        and rows * sp <= 1024
        and sp * tp <= 32
    )
    if fits:
        return fused_layer(*arrays)
    return plain_layer(*arrays)


def solution(mesh):
    return jax.shard_map(
        per_device,
        mesh=mesh,
        in_specs=(
            P("sp", None),
            P("sp", "tp"),
            P("sp", "tp"),
            P("sp", None),
            P("sp", None),
            P(),
            P(None, "tp"),
            P(None, "tp"),
            P("tp", None),
            P(),
            P("sp", "tp"),
            P("sp", "tp"),
            P("tp", "sp"),
        ),
        out_specs=P(("sp", "tp"), None),
        check_vma=False,
    )
```

```python
import functools
import math

import jax
import jax.numpy as jnp
from jax import lax
from jax.experimental import pallas as pl
from jax.experimental.pallas import tpu as pltpu
from jax.sharding import PartitionSpec as P

NOPE = 64
ROPE = 32
V = 64


def rotate(values, cosine, sine):
    half_width = values.shape[-1] // 2
    first = values[..., :half_width]
    second = values[..., half_width:]
    return jnp.concatenate(
        [first * cosine - second * sine, first * sine + second * cosine], axis=-1
    )


def rms_scale(values, gain):
    return values * lax.rsqrt(jnp.mean(values * values, axis=-1, keepdims=True) + 1e-06) * gain


def plain_layer(
    resid_in,
    query_plain,
    query_turn,
    latent_raw,
    shared_key,
    latent_gain,
    key_up,
    value_up,
    out_weight,
    mixer_gain,
    gate_weight,
    up_weight,
    down_weight,
):
    tok_rows = resid_in.shape[0]
    head_count = query_plain.shape[1] // NOPE
    part_rows = tok_rows // lax.axis_size("tp")
    offset = lax.axis_index("sp") * tok_rows
    position = (offset + jnp.arange(tok_rows, dtype=jnp.int32)).astype(jnp.float32)
    inverse = 10000.0 ** (-jnp.arange(0, ROPE, 2, dtype=jnp.float32) / ROPE)
    angles = position[:, None] * inverse[None, :]
    cosine = jnp.cos(angles)
    sine = jnp.sin(angles)
    query_heads = query_plain.reshape(tok_rows, head_count, NOPE)
    query_rot = rotate(
        query_turn.reshape(tok_rows, head_count, ROPE).astype(jnp.float32),
        cosine[:, None, :],
        sine[:, None, :],
    ).astype(jnp.bfloat16)
    latent = rms_scale(latent_raw.astype(jnp.float32), latent_gain).astype(jnp.bfloat16)
    key_rot = rotate(shared_key.astype(jnp.float32), cosine, sine).astype(jnp.bfloat16)
    softmax_scale = (NOPE + ROPE) ** (-0.5)

    def attend_block(state, key_plain, values, key_pos):
        run_max, run_total, run_acc = state
        score = jnp.einsum(
            "qhd,khd->hqk", query_heads, key_plain, preferred_element_type=jnp.float32
        )
        score = score + jnp.einsum(
            "qhr,kr->hqk", query_rot, key_pos, preferred_element_type=jnp.float32
        )
        score = score * softmax_scale
        new_max = jnp.maximum(run_max, jnp.max(score, axis=-1))
        shrink = jnp.exp(run_max - new_max)
        expo = jnp.exp(score - new_max[:, :, None])
        run_total = run_total * shrink + jnp.sum(expo, axis=-1)
        run_acc = run_acc * shrink.T[:, :, None] + jnp.einsum(
            "hqk,khd->qhd", expo.astype(jnp.bfloat16), values, preferred_element_type=jnp.float32
        )
        return (new_max, run_total, run_acc)

    start_state = (
        jnp.full((head_count, tok_rows), -jnp.inf, jnp.float32),
        jnp.zeros((head_count, tok_rows), jnp.float32),
        jnp.zeros((tok_rows, head_count, V), jnp.float32),
    )
    state = start_state
    latent_piece = lax.all_gather(latent, "sp", axis=0, tiled=True)
    pos_piece = lax.all_gather(key_rot, "sp", axis=0, tiled=True)
    piece_len = latent_piece.shape[0]
    block_len = math.gcd(piece_len, 512)
    block_count = piece_len // block_len

    def one_block(inner, items):
        latent_rows, pos_rows = items
        key_plain = (
            jnp.dot(latent_rows, key_up, preferred_element_type=jnp.float32)
            .astype(jnp.bfloat16)
            .reshape(block_len, head_count, NOPE)
        )
        values = (
            jnp.dot(latent_rows, value_up, preferred_element_type=jnp.float32)
            .astype(jnp.bfloat16)
            .reshape(block_len, head_count, V)
        )
        return (attend_block(inner, key_plain, values, pos_rows), None)

    state, unused = lax.scan(
        one_block,
        state,
        (
            latent_piece.reshape(block_count, block_len, latent_piece.shape[1]),
            pos_piece.reshape(block_count, block_len, ROPE),
        ),
    )
    attended = (
        (state[2] / state[1].T[:, :, None]).astype(jnp.bfloat16).reshape(tok_rows, head_count * V)
    )
    own_start = lax.axis_index("tp") * part_rows
    mixed = lax.psum_scatter(
        jnp.dot(attended, out_weight, preferred_element_type=jnp.float32).astype(jnp.bfloat16),
        "tp",
        scatter_dimension=0,
        tiled=True,
    ).astype(jnp.float32)
    middle = lax.dynamic_slice_in_dim(resid_in, own_start, part_rows, 0).astype(jnp.float32) + mixed
    normed = rms_scale(middle, mixer_gain).astype(jnp.bfloat16)
    all_rows = lax.all_gather(normed, "tp", axis=0, tiled=True)
    gate_sum = jnp.dot(
        all_rows,
        lax.all_gather(gate_weight, "sp", axis=0, tiled=True),
        preferred_element_type=jnp.float32,
    )
    up_sum = jnp.dot(
        all_rows,
        lax.all_gather(up_weight, "sp", axis=0, tiled=True),
        preferred_element_type=jnp.float32,
    )
    hidden = (jax.nn.silu(gate_sum) * up_sum).astype(jnp.bfloat16)
    terms = jnp.dot(
        hidden,
        lax.all_gather(down_weight, "sp", axis=1, tiled=True),
        preferred_element_type=jnp.float32,
    )
    down_sum = lax.psum_scatter(
        terms.astype(jnp.bfloat16), "tp", scatter_dimension=0, tiled=True
    ).astype(jnp.float32)
    return (middle + 0.5 * down_sum).astype(jnp.bfloat16)

MESH = pl.DeviceIdType.MESH
BF = jnp.bfloat16
F32 = jnp.float32
BY_LAST = (((1,), (1,)), ((), ()))


def turn(values, cosine, sine):
    width = values.shape[-1]
    half = ROPE // 2
    lane = lax.broadcasted_iota(jnp.int32, values.shape, 1) % ROPE
    swapped = jnp.where(lane < half, pltpu.roll(values, width - half, 1), pltpu.roll(values, half, 1))
    return values * cosine + swapped * sine


def layer_kernel(
    sizes,
    latent_ref,
    shared_ref,
    inv_ref,
    lgain_ref,
    mgain_ref,
    query_hbm,
    turn_hbm,
    kup_hbm,
    vup_hbm,
    ow_hbm,
    resid_hbm,
    gate_hbm,
    up_hbm,
    down_hbm,
    out_ref,
    query_ref,
    turn_ref,
    kup_ref,
    vup_ref,
    ow_ref,
    resid_ref,
    raw_buf,
    wt_buf,
    relay_buf,
    kv_buf,
    key_buf,
    val_buf,
    att_buf,
    mix_buf,
    pair_buf,
    paird_buf,
    cross_buf,
    crossr_buf,
    mid_buf,
    w_buf,
    wd_buf,
    n_buf,
    h_buf,
    acc_buf,
    r_buf,
    load_sem,
    l_ssem,
    l_rsem,
    c_ssem,
    c_rsem,
    f_ssem,
    f_rsem,
    m_ssem,
    m_rsem,
    w_ssem,
    w_rsem,
    y_ssem,
    y_rsem,
    x_ssem,
    x_rsem,
    a_ssem,
    a_rsem,
    s_ssem,
    s_rsem,
):
    sp, tp = sizes
    s = lax.axis_index("sp")
    t = lax.axis_index("tp")
    core = t % 2
    x = t // 2
    y = s % 2
    zl = (s // 2) % 2
    zh = s // 4
    other = t + 1 - 2 * core
    rows = latent_ref.shape[0]
    part = rows // tp
    hid, cols = down_hbm.shape[1:]
    kv_width = latent_ref.shape[1]
    lanes = cols // 2
    quarter = sp // 2 * lanes
    width = ow_hbm.shape[1]
    along_x = (s, (1 - x) * 2 + core)

    def bits(q):
        flip = lambda bit, by: bit + by * (1 - 2 * bit)
        return flip(zh, q // 4), flip(zl, q // 2 % 2), flip(y, q % 2)

    def ring(q):
        high, low, side = bits(q)
        return high * 4 + low * 2 + side

    def place(q):
        high, low, side = bits(q)
        return (1 - high - low + 2 * high * low) * 4 + high * 2 + side

    def remote(src, dst, ssem, rsem, dev):
        return pltpu.make_async_remote_copy(
            src_ref=src, dst_ref=dst, send_sem=ssem, recv_sem=rsem, device_id=dev, device_id_type=MESH
        )

    def send(src, dst, ssem, rsem, dev):
        remote(src, dst, ssem, rsem, dev).start()

    def sent(ref, ssem):
        remote(ref, ref, ssem, ssem, (s, other)).wait_send()

    def arrived(ref, rsem):
        remote(ref, ref, rsem, rsem, (s, other)).wait_recv()

    barrier = pltpu.get_barrier_semaphore()
    for q in range(1, sp):
        pl.semaphore_signal(barrier, inc=1, device_id=(ring(q), t), device_id_type=MESH)
    for j in range(1, tp):
        pl.semaphore_signal(barrier, inc=1, device_id=(s, (t + j) % tp), device_id_type=MESH)
    for q in (2, 4):
        pl.semaphore_signal(barrier, inc=1, device_id=(ring(q), along_x[1]), device_id_type=MESH)

    own_rows = pl.ds(pl.multiple_of(t * part, part), part)
    own_cols = pl.ds(pl.multiple_of(s * cols, cols), cols)
    own_lanes = pl.ds(pl.multiple_of(place(0) * lanes, lanes), lanes)
    loads = [
        pltpu.make_async_copy(src, dst, load_sem.at[i])
        for i, (src, dst) in enumerate(
            [
                (gate_hbm, raw_buf.at[0]),
                (up_hbm, raw_buf.at[1]),
                (kup_hbm, kup_ref),
                (vup_hbm, vup_ref),
                (turn_hbm, turn_ref),
                (query_hbm, query_ref),
                (ow_hbm, ow_ref),
                (resid_hbm.at[own_rows], resid_ref),
                (down_hbm.at[s, :, :lanes], wd_buf.at[0, core, :, own_lanes]),
                (down_hbm.at[s, :, lanes:], wd_buf.at[1, core, :, own_lanes]),
                (down_hbm, wt_buf.at[2]),
            ]
        )
    ]
    for load in loads:
        load.start()

    position = (s * rows + lax.broadcasted_iota(jnp.int32, (rows, 128), 0)).astype(F32)
    angles = position * inv_ref[...]
    sign = jnp.where(lax.broadcasted_iota(jnp.int32, (rows, 128), 1) % ROPE < ROPE // 2, -1.0, 1.0)
    cosine = jnp.cos(angles)
    sine = jnp.sin(angles) * sign
    lat = latent_ref[...].astype(F32)
    lat = lat * lax.rsqrt(jnp.mean(lat * lat, axis=-1, keepdims=True) + 1e-06) * lgain_ref[...]
    own_lat = lat.astype(BF)
    shared = shared_ref[...].astype(F32)
    shared = jnp.concatenate([shared] * (128 // ROPE), axis=0).T
    own_key = turn(shared, cosine, sine).astype(BF)
    for j in range(tp):
        part_of = slice(j * part, (j + 1) * part)
        kv_buf[0, j, :, :kv_width] = own_lat[part_of]
        kv_buf[0, j, :, kv_width:] = own_key[part_of]

    pl.semaphore_wait(barrier, sp - 1 + tp + 1)

    along_y = (ring(1), t)

    def send_latent(slot, by):
        to = slot + by
        send(kv_buf.at[slot, t], kv_buf.at[to, t], l_ssem.at[0], l_rsem.at[to], (ring(by), t))

    for by in (6, 4, 2, 1):
        send_latent(0, by)

    for which in range(2):
        loads[which].wait()
        turned_buf = wt_buf.at[which].reshape(sp * hid, cols)
        for j in range(raw_buf.shape[2] // 128):
            tile = slice(j * 128, (j + 1) * 128)
            turned_buf[tile, :] = raw_buf[which, :, tile].T

    first = (
        [(0, 2), (0, 6), (1, 2), (1, 6), (0, 4)],
        [(0, 2), (1, 2), (0, 6), (1, 6), (0, 4), (1, 4)],
    )
    between = ([], [(0, 7)])
    second = ([], [(1, 7)])
    third = (
        [(1, 4), (0, 3), (0, 7), (1, 3), (1, 7), (0, 5), (1, 5)],
        [(0, 3), (1, 3), (0, 5), (1, 5)],
    )
    fourth = [(w, q) for w in (2, 3) for q in (2, 3, 6, 7, 4, 5)]
    role = 1 - zh - zl + 2 * zh * zl
    outer = role == 1

    def late(which, q):
        return int(q in (7, 5, 3)) if which < 2 else role

    def weight_slot(which, q, side=core):
        if which < 2:
            return w_buf.at[which, side, :, pl.ds(pl.multiple_of(ring(q) * cols, cols), cols)]
        return wd_buf.at[which - 2, side, :, pl.ds(pl.multiple_of(place(q) * lanes, lanes), lanes)]

    def lanes_of(ref, which):
        return ref if which < 2 else ref.at[:, (which - 2) * lanes:(which - 1) * lanes]

    def send_weights(some):
        for which, q in some:
            kind = min(which, 2)
            if q > 1 and q % 2:
                src, owner, dest = relay_buf.at[kind, q // 2 - 1], 1, (ring(q - 1), t)
            else:
                src, owner, dest = wt_buf.at[kind, ring(q)], 0, (ring(q), t)
            send(
                lanes_of(src, which),
                weight_slot(which, owner),
                w_ssem.at[which],
                w_rsem.at[which, late(which, q)],
                dest,
            )

    def send_relays(kind):
        for q in (7, 5, 3):
            send(
                wt_buf.at[kind, ring(q)], relay_buf.at[kind, q // 2 - 1], y_ssem.at[kind], y_rsem.at[kind], along_y
            )
        send_weights([(which, 1) for which in ((kind,) if kind < 2 else (2, 3))])

    def relayed(kind):
        arrived(relay_buf.at[kind], y_rsem.at[kind])

    def send_by_place(lists):
        @pl.when(outer)
        def _():
            send_weights(lists[0])

        @pl.when(jnp.logical_not(outer))
        def _():
            send_weights(lists[1])

    def some_of(which, side, count):
        if which < 2:
            return w_buf.at[which, side, :, :count * cols]
        return wd_buf.at[which - 2, side, :, :count * lanes]

    def pass_on(which, some, index):
        for q in some:
            slot = weight_slot(which, q)
            send(slot, slot, x_ssem.at[index], x_rsem.at[index], (s, other))

    def pass_weights(which, group):
        some = [q for q in range(1, sp) if late(which, q) == group]
        arrived(some_of(which, core, len(some)), w_rsem.at[which, group])
        pass_on(which, [0] * (1 - group) + some, which)

    def passed_weights(which):
        arrived(some_of(which, 1 - core, sp), x_rsem.at[which])

    def pass_down(q):
        h, c = q // 2, q % 2

        @pl.when(role == c)
        def _():
            arrived(some_of(2 + h, core, sp // 2 - 1), w_rsem.at[2 + h, c])
            pass_on(2 + h, (0, 1, 6, 7), 2 + q)

        @pl.when(role != c)
        def _():
            arrived(some_of(2 + h, core, sp // 2), w_rsem.at[2 + h, c])
            pass_on(2 + h, (2, 3, 4, 5), 2 + q)

    def passed_down(q):
        arrived(some_of(2 + q // 2, 1 - core, sp // 2), x_rsem.at[2 + q])

    send_relays(0)
    send_relays(1)
    for which in range(2):
        w_buf[which, core, :, own_cols] = wt_buf[which, s]

    def make_kv(k):
        piece = kv_buf[k].reshape(rows, kv_buf.shape[3])
        piece_lat = piece[:, :kv_width]
        key_buf[k * rows:(k + 1) * rows, :] = jnp.dot(
            piece_lat, kup_ref[...], preferred_element_type=F32
        ).astype(BF)
        val_buf[k * rows:(k + 1) * rows, :] = jnp.dot(
            piece_lat, vup_ref[...], preferred_element_type=F32
        ).astype(BF)

    for load in loads[2:10]:
        load.wait()
    make_kv(0)
    query_rot = turn(
        turn_ref[...].astype(F32),
        jnp.concatenate([cosine] * (turn_ref.shape[1] // 128), axis=1),
        jnp.concatenate([sine] * (turn_ref.shape[1] // 128), axis=1),
    ).astype(BF)

    def pass_latent(slot, quarter):
        piece = kv_buf.at[slot, quarter]
        send(piece, piece, f_ssem.at[0], f_rsem.at[slot], (s, other))

    def take_latent(slot):
        piece = kv_buf.at[slot, t]
        arrived(piece, l_rsem.at[slot])
        send(piece, piece, c_ssem.at[0], c_rsem.at[slot], along_x)
        pass_latent(slot, t)

    take_latent(1)
    for by in (6, 4, 2):
        send_latent(1, by)
    loads[10].wait()
    send_relays(2)
    order = (2, 4, 6, 3, 5, 7)
    for slot in order:
        take_latent(slot)
    send_by_place(first)
    def take_block(slot):
        arrived(kv_buf.at[slot, pl.ds(0, tp // 2)], f_rsem.at[slot])
        make_kv(slot)

    order = (1,) + order
    for i, slot in enumerate(order):
        arrived(kv_buf.at[slot, along_x[1]], c_rsem.at[slot])
        pass_latent(slot, along_x[1])
        if i > 1:
            take_block(order[i - 2])
    for slot in order[-2:]:
        take_block(slot)

    scale = (NOPE + ROPE) ** (-0.5) * math.log2(math.e)
    all_rot = kv_buf[...].reshape(sp * rows, kv_buf.shape[3])[:, kv_width:]
    lane = lax.broadcasted_iota(jnp.int32, (rows, 128), 1)
    for pair in range(query_ref.shape[1] // 128):
        span = slice(pair * 128, (pair + 1) * 128)
        keys = jnp.concatenate([key_buf[:, span], all_rot], axis=1)
        vals = val_buf[:, span]
        results = []
        for inner in range(2):
            head = pair * 2 + inner
            tile = head * ROPE // 128
            group = head % (128 // ROPE)
            q_plain = jnp.where(lane // NOPE == inner, query_ref[:, span], jnp.zeros((), BF))
            q_turn = jnp.where(
                lane // ROPE == group, query_rot[:, tile * 128:(tile + 1) * 128], jnp.zeros((), BF)
            )
            score = lax.dot_general(
                jnp.concatenate([q_plain, q_turn], axis=1), keys, BY_LAST, preferred_element_type=F32
            )
            top = jnp.max(score, axis=-1, keepdims=True)
            expo = jnp.exp2((score - top) * scale)
            total = jnp.sum(expo, axis=-1, keepdims=True)
            results.append(jnp.dot(expo.astype(BF), vals, preferred_element_type=F32) / total)
        att_buf[:, span] = jnp.where(lane < V, results[0], results[1]).astype(BF)

    relayed(0)
    send_by_place(between)
    span_of = [slice(c * width // 2, (c + 1) * width // 2) for c in range(2)]
    for c, span in enumerate(span_of):
        mix = jnp.dot(att_buf[...], ow_ref[:, span], preferred_element_type=F32)
        mix_buf[:, span] = mix
        for dest in range(tp):
            pair_buf[dest % 2, c, dest // 2] = mix[dest * part:(dest + 1) * part].astype(BF)
        send(pair_buf.at[1 - core, c], paird_buf.at[c], m_ssem.at[c], m_rsem.at[c], (s, other))
    cross_rows = pl.ds(pl.multiple_of(((1 - x) * 2 + core) * part, part), part)
    for c, span in enumerate(span_of):
        arrived(paird_buf.at[c], m_rsem.at[c])
        cross_buf[c] = (mix_buf[cross_rows, span] + paird_buf[c, 1 - x].astype(F32)).astype(BF)
        send(cross_buf.at[c], crossr_buf.at[c], m_ssem.at[2 + c], m_rsem.at[2 + c], along_x)
    mids = [
        resid_ref[:, span].astype(F32) + mix_buf[own_rows, span] + paird_buf[c, x].astype(F32)
        for c, span in enumerate(span_of)
    ]
    for c in range(2):
        arrived(crossr_buf.at[c], m_rsem.at[2 + c])
        mids[c] = mids[c] + crossr_buf[c].astype(F32)
    mid = jnp.concatenate(mids, axis=1)
    mid_buf[...] = mid
    normed = mid * lax.rsqrt(jnp.mean(mid * mid, axis=-1, keepdims=True) + 1e-06) * mgain_ref[...]
    n_buf[0] = normed.astype(BF)

    a_x = 1 - core
    pick = lambda first_x, i: first_x * along_x[i] + (1 - first_x) * along_y[i]
    steps = (
        (8, (pick(a_x, 0), pick(a_x, 1))),
        (4, (pick(core, 0), pick(core, 1))),
        (2, (ring(2), t)),
        (1, (ring(4), t)),
    )

    def spread(slot):
        for by, dev in reversed(steps):
            if by > slot:
                to = slot + by
                send(n_buf.at[slot], n_buf.at[to], a_ssem.at[0], a_rsem.at[min(to, sp)], dev)

    spread(0)
    relayed(1)
    send_by_place(second)
    arrived(n_buf.at[1], a_rsem.at[1])
    spread(1)
    send_by_place(third)
    relayed(2)
    send_weights(fourth)
    for slot in (2, 3):
        arrived(n_buf.at[slot], a_rsem.at[slot])
        spread(slot)
    for slot in (4, 5, 6, 7):
        arrived(n_buf.at[slot], a_rsem.at[slot])
        spread(slot)
    pass_weights(0, 0)
    pass_weights(1, 0)
    pass_weights(0, 1)
    pass_weights(1, 1)
    group = n_buf.shape[0] // 2

    def hidden_of(side):
        for g in range(2):
            block = n_buf[g * group:(g + 1) * group].reshape(group * part, width)
            gate = lax.dot_general(block, w_buf[0, side], BY_LAST, preferred_element_type=F32)
            up = lax.dot_general(block, w_buf[1, side], BY_LAST, preferred_element_type=F32)
            hidden = (gate / (1.0 + jnp.exp(-gate)) * up).astype(BF)
            for k in range(group):
                slot = k % 2 * 8 + g * 4 + k // 2 % 2 * 2 + k // 4
                h_buf[side, slot * part:(slot + 1) * part, :] = hidden[k * part:(k + 1) * part]

    arrived(n_buf.at[pl.ds(group, group)], a_rsem.at[sp])
    hidden_of(core)
    passed_weights(0)
    passed_weights(1)
    hidden_of(1 - core)

    last = (3,)
    to_first, to_second, to_low, to_high = (dev for by, dev in steps)
    messages = {
        14: (2, to_first),
        12: (2, to_first),
        10: (2, to_low),
        9: (1, to_second),
        8: (1, to_high),
        6: (2, to_first),
        4: (2, to_first),
        2: (2, to_low),
        1: (1, to_second),
    }
    index_of = {slot: i for i, slot in enumerate((*messages, 3))}

    def over(q):
        return (ring(q + 1 - core), t + core * (along_x[1] - t))

    direct = {**messages, 3: (1, over(2)), 2: (1, to_low), 9: (1, over(4))}

    def message(q, slot):
        return direct[slot] if q in last else messages[slot]

    def sums(q, slot):
        count, dev = message(q, slot)
        some = pl.ds(slot, count)
        send(acc_buf.at[q, some], r_buf.at[q, some], s_ssem.at[q], s_rsem.at[q, index_of[slot]], dev)

    def project(q):
        h, columns = q // 2, slice(q % 2 * quarter, (q % 2 + 1) * quarter)
        for g in (1, 0):
            span = slice(g * group * part, (g + 1) * group * part)
            down = jnp.dot(
                h_buf[0, span], wd_buf[h, 0, :, columns], preferred_element_type=F32
            ) + jnp.dot(h_buf[1, span], wd_buf[h, 1, :, columns], preferred_element_type=F32)
            acc_buf[q, g * group:(g + 1) * group] = down.astype(BF).reshape(group, part, quarter)
            sums(q, g * group + 6)
            sums(q, g * group + 4)

    def landed(q, slot):
        count = message(q, slot)[0]
        arrived(r_buf.at[q, pl.ds(slot, count)], s_rsem.at[q, index_of[slot]])
        return r_buf[q, slot:slot + count].astype(F32)

    def join(q, to, *slots):
        count = message(q, slots[0])[0]
        value = acc_buf[q, to:to + count].astype(F32)
        for slot in slots:
            value = value + landed(q, slot)
        acc_buf[q, to:to + count] = value.astype(BF)

    def to_10(q):
        join(q, 10, 14)
        sums(q, 10)

    def to_2(q):
        join(q, 2, 6)
        if q in last:
            sums(q, 3)
        sums(q, 2)

    def to_9(q):
        join(q, 8, 12, 10)
        sums(q, 9)
        if q in last:
            sums(q, 8)

    def to_8(q):
        if q not in last:
            join(q, 8, 9)
            sums(q, 8)

    def to_1(q):
        join(q, 0, *((4,) if q in last else (4, 2)))
        sums(q, 1)

    def finish(q):
        value = acc_buf[q, 0].astype(F32)
        for slot in (2, 3, 9, 1, 8) if q in last else (1, 8):
            value = value + landed(q, slot)[0]
        h, c = q // 2, q % 2
        for k in range(sp // 2):
            z = (1 + k // 2) if c == 0 else 3 * (k // 2)
            start = (2 * z + k % 2) * cols + h * lanes
            span = slice(start, start + lanes)
            out_ref[:, span] = (
                mid_buf[:, span] + 0.5 * value[:, k * lanes:(k + 1) * lanes]
            ).astype(BF)

    pass_down(0)
    passed_down(0)
    project(0)
    pass_down(1)
    passed_down(1)
    project(1)
    to_10(0)
    to_2(0)
    pass_down(2)
    passed_down(2)
    project(2)
    to_10(1)
    to_9(0)
    to_2(1)
    pass_down(3)
    passed_down(3)
    project(3)
    to_9(1)
    to_10(2)
    to_2(2)
    to_8(0)
    to_10(3)
    to_8(1)
    to_9(2)
    to_2(3)
    to_1(0)
    to_1(1)
    to_8(2)
    to_9(3)
    to_1(2)
    to_1(3)
    finish(0)
    finish(1)
    finish(2)
    finish(3)

    for h in range(4):
        sent(r_buf.at[h, pl.ds(1, 2 * sp - 1)], s_ssem.at[h])
    sent(n_buf.at[pl.ds(1, 2 * sp - 1)], a_ssem.at[0])
    for c in range(2):
        sent(paird_buf.at[c], m_ssem.at[c])
        sent(crossr_buf.at[c], m_ssem.at[2 + c])
    sent(kv_buf.at[pl.ds(1, sp - 1), 0], l_ssem.at[0])
    sent(kv_buf.at[pl.ds(1, sp - 1), 0], c_ssem.at[0])
    sent(kv_buf.at[pl.ds(1, sp - 1), pl.ds(0, tp // 2)], f_ssem.at[0])
    for kind in range(3):
        sent(relay_buf.at[kind], y_ssem.at[kind])
    for which in range(4):
        sent(some_of(which, core, sp - 1), w_ssem.at[which])
    for which in range(2):
        sent(some_of(which, core, sp), x_ssem.at[which])
        for c in range(2):
            sent(some_of(2 + which, core, sp // 2), x_ssem.at[2 + 2 * which + c])


def fused_layer(
    resid_in,
    query_plain,
    query_turn,
    latent_raw,
    shared_key,
    latent_gain,
    key_up,
    value_up,
    out_weight,
    mixer_gain,
    gate_weight,
    up_weight,
    down_weight,
):
    sp = lax.axis_size("sp")
    tp = lax.axis_size("tp")
    rows, width = resid_in.shape
    part = rows // tp
    hid = down_weight.shape[0] // sp
    cols = down_weight.shape[1]
    kv = latent_raw.shape[1]
    heads_width = query_plain.shape[1]
    inverse = 10000.0 ** (-jnp.arange(0, ROPE, 2, dtype=F32) / ROPE)
    inverse_lanes = jnp.tile(inverse, 128 * 2 // ROPE)[None, :]
    chips = sp * tp // 2
    dma = pltpu.SemaphoreType.DMA
    vmem = lambda *shape: pltpu.VMEM(shape, BF)
    near = pl.BlockSpec(memory_space=pltpu.VMEM)
    far = pl.BlockSpec(memory_space=pl.ANY)
    return pl.pallas_call(
        functools.partial(layer_kernel, (sp, tp)),
        out_shape=pltpu.VMEM((part, width), BF),
        in_specs=[near] * 5 + [far] * 9,
        out_specs=near,
        scratch_shapes=[
            vmem(*query_plain.shape),
            vmem(*query_turn.shape),
            vmem(*key_up.shape),
            vmem(*value_up.shape),
            vmem(*out_weight.shape),
            vmem(part, width),
            vmem(2, *gate_weight.shape),
            vmem(3, sp, hid, cols),
            vmem(3, sp // 2 - 1, hid, cols),
            vmem(sp, tp, part, kv + 128),
            vmem(sp * rows, heads_width),
            vmem(sp * rows, heads_width),
            vmem(rows, heads_width),
            pltpu.VMEM((rows, width), F32),
            vmem(2, 2, tp // 2, part, width // 2),
            vmem(2, tp // 2, part, width // 2),
            vmem(2, part, width // 2),
            vmem(2, part, width // 2),
            pltpu.VMEM((part, width), F32),
            vmem(2, 2, hid, width),
            vmem(2, 2, hid, width // 2),
            vmem(chips, part, width),
            vmem(2, chips * part, hid),
            vmem(4, chips, part, width // 4),
            vmem(4, chips, part, width // 4),
            dma((11,)),
            dma((1,)),
            dma((sp,)),
            dma((1,)),
            dma((sp,)),
            dma((1,)),
            dma((sp,)),
            dma((4,)),
            dma((4,)),
            dma((4,)),
            dma((4, 2)),
            dma((3,)),
            dma((3,)),
            dma((6,)),
            dma((6,)),
            dma((1,)),
            dma((sp + 1,)),
            dma((4,)),
            dma((4, sp + 2)),
        ],
        compiler_params=pltpu.CompilerParams(
            collective_id=0, has_side_effects=True, vmem_limit_bytes=60 * 1024 * 1024
        ),
    )(
        latent_raw,
        shared_key.T,
        inverse_lanes,
        latent_gain[None, :],
        mixer_gain[None, :],
        query_plain,
        query_turn,
        key_up,
        value_up,
        out_weight,
        resid_in,
        gate_weight,
        up_weight,
        down_weight.reshape(sp, hid, cols),
    )


def per_device(*arrays):
    resid_in, query_plain, query_turn, latent_raw = arrays[:4]
    down_weight = arrays[-1]
    sp = lax.axis_size("sp")
    tp = lax.axis_size("tp")
    rows = resid_in.shape[0]
    fits = (
        sp // 4 == 2
        and tp // 2 == 2
        and rows % (32 * tp) == 0
        and down_weight.shape[0] % (16 * sp) == 0
        and down_weight.shape[1] % 128 == 0
        and latent_raw.shape[1] % 128 == 0
        and query_plain.shape[1] % 128 == 0
        and query_turn.shape[1] % 128 == 0
        and rows * sp <= 1024
        and sp * tp <= 32
    )
    if fits:
        return fused_layer(*arrays)
    return plain_layer(*arrays)


def solution(mesh):
    return jax.shard_map(
        per_device,
        mesh=mesh,
        in_specs=(
            P("sp", None),
            P("sp", "tp"),
            P("sp", "tp"),
            P("sp", None),
            P("sp", None),
            P(),
            P(None, "tp"),
            P(None, "tp"),
            P("tp", None),
            P(),
            P("sp", "tp"),
            P("sp", "tp"),
            P("tp", "sp"),
        ),
        out_specs=P(("sp", "tp"), None),
        check_vma=False,
    )
```

```python
import functools
import math

import jax
import jax.numpy as jnp
from jax import lax
from jax.experimental import pallas as pl
from jax.experimental.pallas import tpu as pltpu
from jax.sharding import PartitionSpec as P

NOPE = 64
ROPE = 32
V = 64


def rotate(values, cosine, sine):
    half_width = values.shape[-1] // 2
    first = values[..., :half_width]
    second = values[..., half_width:]
    return jnp.concatenate(
        [first * cosine - second * sine, first * sine + second * cosine], axis=-1
    )


def rms_scale(values, gain):
    return values * lax.rsqrt(jnp.mean(values * values, axis=-1, keepdims=True) + 1e-06) * gain


def plain_layer(
    resid_in,
    query_plain,
    query_turn,
    latent_raw,
    shared_key,
    latent_gain,
    key_up,
    value_up,
    out_weight,
    mixer_gain,
    gate_weight,
    up_weight,
    down_weight,
):
    tok_rows = resid_in.shape[0]
    head_count = query_plain.shape[1] // NOPE
    part_rows = tok_rows // lax.axis_size("tp")
    offset = lax.axis_index("sp") * tok_rows
    position = (offset + jnp.arange(tok_rows, dtype=jnp.int32)).astype(jnp.float32)
    inverse = 10000.0 ** (-jnp.arange(0, ROPE, 2, dtype=jnp.float32) / ROPE)
    angles = position[:, None] * inverse[None, :]
    cosine = jnp.cos(angles)
    sine = jnp.sin(angles)
    query_heads = query_plain.reshape(tok_rows, head_count, NOPE)
    query_rot = rotate(
        query_turn.reshape(tok_rows, head_count, ROPE).astype(jnp.float32),
        cosine[:, None, :],
        sine[:, None, :],
    ).astype(jnp.bfloat16)
    latent = rms_scale(latent_raw.astype(jnp.float32), latent_gain).astype(jnp.bfloat16)
    key_rot = rotate(shared_key.astype(jnp.float32), cosine, sine).astype(jnp.bfloat16)
    softmax_scale = (NOPE + ROPE) ** (-0.5)

    def attend_block(state, key_plain, values, key_pos):
        run_max, run_total, run_acc = state
        score = jnp.einsum(
            "qhd,khd->hqk", query_heads, key_plain, preferred_element_type=jnp.float32
        )
        score = score + jnp.einsum(
            "qhr,kr->hqk", query_rot, key_pos, preferred_element_type=jnp.float32
        )
        score = score * softmax_scale
        new_max = jnp.maximum(run_max, jnp.max(score, axis=-1))
        shrink = jnp.exp(run_max - new_max)
        expo = jnp.exp(score - new_max[:, :, None])
        run_total = run_total * shrink + jnp.sum(expo, axis=-1)
        run_acc = run_acc * shrink.T[:, :, None] + jnp.einsum(
            "hqk,khd->qhd", expo.astype(jnp.bfloat16), values, preferred_element_type=jnp.float32
        )
        return (new_max, run_total, run_acc)

    start_state = (
        jnp.full((head_count, tok_rows), -jnp.inf, jnp.float32),
        jnp.zeros((head_count, tok_rows), jnp.float32),
        jnp.zeros((tok_rows, head_count, V), jnp.float32),
    )
    state = start_state
    latent_piece = lax.all_gather(latent, "sp", axis=0, tiled=True)
    pos_piece = lax.all_gather(key_rot, "sp", axis=0, tiled=True)
    piece_len = latent_piece.shape[0]
    block_len = math.gcd(piece_len, 512)
    block_count = piece_len // block_len

    def one_block(inner, items):
        latent_rows, pos_rows = items
        key_plain = (
            jnp.dot(latent_rows, key_up, preferred_element_type=jnp.float32)
            .astype(jnp.bfloat16)
            .reshape(block_len, head_count, NOPE)
        )
        values = (
            jnp.dot(latent_rows, value_up, preferred_element_type=jnp.float32)
            .astype(jnp.bfloat16)
            .reshape(block_len, head_count, V)
        )
        return (attend_block(inner, key_plain, values, pos_rows), None)

    state, unused = lax.scan(
        one_block,
        state,
        (
            latent_piece.reshape(block_count, block_len, latent_piece.shape[1]),
            pos_piece.reshape(block_count, block_len, ROPE),
        ),
    )
    attended = (
        (state[2] / state[1].T[:, :, None]).astype(jnp.bfloat16).reshape(tok_rows, head_count * V)
    )
    own_start = lax.axis_index("tp") * part_rows
    mixed = lax.psum_scatter(
        jnp.dot(attended, out_weight, preferred_element_type=jnp.float32).astype(jnp.bfloat16),
        "tp",
        scatter_dimension=0,
        tiled=True,
    ).astype(jnp.float32)
    middle = lax.dynamic_slice_in_dim(resid_in, own_start, part_rows, 0).astype(jnp.float32) + mixed
    normed = rms_scale(middle, mixer_gain).astype(jnp.bfloat16)
    all_rows = lax.all_gather(normed, "tp", axis=0, tiled=True)
    gate_sum = jnp.dot(
        all_rows,
        lax.all_gather(gate_weight, "sp", axis=0, tiled=True),
        preferred_element_type=jnp.float32,
    )
    up_sum = jnp.dot(
        all_rows,
        lax.all_gather(up_weight, "sp", axis=0, tiled=True),
        preferred_element_type=jnp.float32,
    )
    hidden = (jax.nn.silu(gate_sum) * up_sum).astype(jnp.bfloat16)
    terms = jnp.dot(
        hidden,
        lax.all_gather(down_weight, "sp", axis=1, tiled=True),
        preferred_element_type=jnp.float32,
    )
    down_sum = lax.psum_scatter(
        terms.astype(jnp.bfloat16), "tp", scatter_dimension=0, tiled=True
    ).astype(jnp.float32)
    return (middle + 0.5 * down_sum).astype(jnp.bfloat16)

MESH = pl.DeviceIdType.MESH
BF = jnp.bfloat16
F32 = jnp.float32
BY_LAST = (((1,), (1,)), ((), ()))


def turn(values, cosine, sine):
    width = values.shape[-1]
    half = ROPE // 2
    lane = lax.broadcasted_iota(jnp.int32, values.shape, 1) % ROPE
    swapped = jnp.where(lane < half, pltpu.roll(values, width - half, 1), pltpu.roll(values, half, 1))
    return values * cosine + swapped * sine


def layer_kernel(
    sizes,
    latent_ref,
    shared_ref,
    inv_ref,
    lgain_ref,
    mgain_ref,
    query_hbm,
    turn_hbm,
    kup_hbm,
    vup_hbm,
    ow_hbm,
    resid_hbm,
    gate_hbm,
    up_hbm,
    down_hbm,
    out_ref,
    query_ref,
    turn_ref,
    kup_ref,
    vup_ref,
    ow_ref,
    resid_ref,
    raw_buf,
    wt_buf,
    relay_buf,
    kv_buf,
    key_buf,
    val_buf,
    att_buf,
    mix_buf,
    pair_buf,
    paird_buf,
    cross_buf,
    crossr_buf,
    mid_buf,
    w_buf,
    wd_buf,
    n_buf,
    h_buf,
    acc_buf,
    r_buf,
    load_sem,
    l_ssem,
    l_rsem,
    c_ssem,
    c_rsem,
    f_ssem,
    f_rsem,
    m_ssem,
    m_rsem,
    w_ssem,
    w_rsem,
    y_ssem,
    y_rsem,
    x_ssem,
    x_rsem,
    a_ssem,
    a_rsem,
    s_ssem,
    s_rsem,
):
    sp, tp = sizes
    s = lax.axis_index("sp")
    t = lax.axis_index("tp")
    core = t % 2
    x = t // 2
    y = s % 2
    zl = (s // 2) % 2
    zh = s // 4
    other = t + 1 - 2 * core
    rows = latent_ref.shape[0]
    part = rows // tp
    hid, cols = down_hbm.shape[1:]
    kv_width = latent_ref.shape[1]
    lanes = cols // 2
    quarter = sp // 2 * lanes
    width = ow_hbm.shape[1]
    along_x = (s, (1 - x) * 2 + core)

    def bits(q):
        flip = lambda bit, by: bit + by * (1 - 2 * bit)
        return flip(zh, q // 4), flip(zl, q // 2 % 2), flip(y, q % 2)

    def ring(q):
        high, low, side = bits(q)
        return high * 4 + low * 2 + side

    def place(q):
        high, low, side = bits(q)
        return (1 - high - low + 2 * high * low) * 4 + high * 2 + side

    def remote(src, dst, ssem, rsem, dev):
        return pltpu.make_async_remote_copy(
            src_ref=src, dst_ref=dst, send_sem=ssem, recv_sem=rsem, device_id=dev, device_id_type=MESH
        )

    def send(src, dst, ssem, rsem, dev):
        remote(src, dst, ssem, rsem, dev).start()

    def sent(ref, ssem):
        remote(ref, ref, ssem, ssem, (s, other)).wait_send()

    def arrived(ref, rsem):
        remote(ref, ref, rsem, rsem, (s, other)).wait_recv()

    barrier = pltpu.get_barrier_semaphore()
    for q in range(1, sp):
        pl.semaphore_signal(barrier, inc=1, device_id=(ring(q), t), device_id_type=MESH)
    for j in range(1, tp):
        pl.semaphore_signal(barrier, inc=1, device_id=(s, (t + j) % tp), device_id_type=MESH)
    for q in (2, 4):
        pl.semaphore_signal(barrier, inc=1, device_id=(ring(q), along_x[1]), device_id_type=MESH)

    own_rows = pl.ds(pl.multiple_of(t * part, part), part)
    own_cols = pl.ds(pl.multiple_of(s * cols, cols), cols)
    own_lanes = pl.ds(pl.multiple_of(place(0) * lanes, lanes), lanes)
    loads = [
        pltpu.make_async_copy(src, dst, load_sem.at[i])
        for i, (src, dst) in enumerate(
            [
                (gate_hbm, raw_buf.at[0]),
                (up_hbm, raw_buf.at[1]),
                (kup_hbm, kup_ref),
                (vup_hbm, vup_ref),
                (turn_hbm, turn_ref),
                (query_hbm, query_ref),
                (ow_hbm, ow_ref),
                (resid_hbm.at[own_rows], resid_ref),
                (down_hbm.at[s, :, :lanes], wd_buf.at[0, core, :, own_lanes]),
                (down_hbm.at[s, :, lanes:], wd_buf.at[1, core, :, own_lanes]),
                (down_hbm, wt_buf.at[2]),
            ]
        )
    ]
    for load in loads:
        load.start()

    position = (s * rows + lax.broadcasted_iota(jnp.int32, (rows, 128), 0)).astype(F32)
    angles = position * inv_ref[...]
    sign = jnp.where(lax.broadcasted_iota(jnp.int32, (rows, 128), 1) % ROPE < ROPE // 2, -1.0, 1.0)
    cosine = jnp.cos(angles)
    sine = jnp.sin(angles) * sign
    lat = latent_ref[...].astype(F32)
    lat = lat * lax.rsqrt(jnp.mean(lat * lat, axis=-1, keepdims=True) + 1e-06) * lgain_ref[...]
    own_lat = lat.astype(BF)
    shared = shared_ref[...].astype(F32)
    shared = jnp.concatenate([shared] * (128 // ROPE), axis=0).T
    own_key = turn(shared, cosine, sine).astype(BF)
    for j in range(tp):
        part_of = slice(j * part, (j + 1) * part)
        kv_buf[0, j, :, :kv_width] = own_lat[part_of]
        kv_buf[0, j, :, kv_width:] = own_key[part_of]

    pl.semaphore_wait(barrier, sp - 1 + tp + 1)

    along_y = (ring(1), t)

    def send_latent(slot, by):
        to = slot + by
        send(kv_buf.at[slot, t], kv_buf.at[to, t], l_ssem.at[0], l_rsem.at[to], (ring(by), t))

    for by in (6, 4, 2, 1):
        send_latent(0, by)

    for which in range(2):
        loads[which].wait()
        turned_buf = wt_buf.at[which].reshape(sp * hid, cols)
        for j in range(raw_buf.shape[2] // 128):
            tile = slice(j * 128, (j + 1) * 128)
            turned_buf[tile, :] = raw_buf[which, :, tile].T

    first = (
        [(0, 2), (0, 6), (1, 2), (1, 6), (0, 4)],
        [(0, 2), (1, 2), (0, 6), (1, 6), (0, 4), (1, 4)],
    )
    between = ([], [(0, 7)])
    second = ([], [(1, 7)])
    third = (
        [(1, 4), (0, 3), (0, 7), (1, 3), (1, 7), (0, 5), (1, 5)],
        [(0, 3), (1, 3), (0, 5), (1, 5)],
    )
    fourth = [(w, q) for w in (2, 3) for q in (2, 3, 6, 7, 4, 5)]
    role = 1 - zh - zl + 2 * zh * zl
    outer = role == 1

    def late(which, q):
        return int(q in (7, 5, 3)) if which < 2 else role

    def weight_slot(which, q, side=core):
        if which < 2:
            return w_buf.at[which, side, :, pl.ds(pl.multiple_of(ring(q) * cols, cols), cols)]
        return wd_buf.at[which - 2, side, :, pl.ds(pl.multiple_of(place(q) * lanes, lanes), lanes)]

    def lanes_of(ref, which):
        return ref if which < 2 else ref.at[:, (which - 2) * lanes:(which - 1) * lanes]

    def send_weights(some):
        for which, q in some:
            kind = min(which, 2)
            if q > 1 and q % 2:
                src, owner, dest = relay_buf.at[kind, q // 2 - 1], 1, (ring(q - 1), t)
            else:
                src, owner, dest = wt_buf.at[kind, ring(q)], 0, (ring(q), t)
            send(
                lanes_of(src, which),
                weight_slot(which, owner),
                w_ssem.at[which // 2],
                w_rsem.at[which, late(which, q)],
                dest,
            )

    def send_relays(kind):
        for q in (7, 5, 3):
            send(
                wt_buf.at[kind, ring(q)], relay_buf.at[kind, q // 2 - 1], y_ssem.at[0], y_rsem.at[kind], along_y
            )
        send_weights([(which, 1) for which in ((kind,) if kind < 2 else (2, 3))])

    def relayed(kind):
        arrived(relay_buf.at[kind], y_rsem.at[kind])

    def send_by_place(lists):
        @pl.when(outer)
        def _():
            send_weights(lists[0])

        @pl.when(jnp.logical_not(outer))
        def _():
            send_weights(lists[1])

    def some_of(which, side, count):
        if which < 2:
            return w_buf.at[which, side, :, :count * cols]
        return wd_buf.at[which - 2, side, :, :count * lanes]

    def pass_on(which, some, index):
        for q in some:
            slot = weight_slot(which, q)
            send(slot, slot, x_ssem.at[which // 2], x_rsem.at[index], (s, other))

    def pass_weights(which, group):
        some = [q for q in range(1, sp) if late(which, q) == group]
        arrived(some_of(which, core, len(some)), w_rsem.at[which, group])
        pass_on(which, [0] * (1 - group) + some, which)

    def passed_weights(which):
        arrived(some_of(which, 1 - core, sp), x_rsem.at[which])

    def pass_down(q):
        h, c = q // 2, q % 2

        @pl.when(role == c)
        def _():
            arrived(some_of(2 + h, core, sp // 2 - 1), w_rsem.at[2 + h, c])
            pass_on(2 + h, (0, 1, 6, 7), 2 + q)

        @pl.when(role != c)
        def _():
            arrived(some_of(2 + h, core, sp // 2), w_rsem.at[2 + h, c])
            pass_on(2 + h, (2, 3, 4, 5), 2 + q)

    def passed_down(q):
        arrived(some_of(2 + q // 2, 1 - core, sp // 2), x_rsem.at[2 + q])

    send_relays(0)
    send_relays(1)
    for which in range(2):
        w_buf[which, core, :, own_cols] = wt_buf[which, s]

    def make_kv(k):
        piece = kv_buf[k].reshape(rows, kv_buf.shape[3])
        piece_lat = piece[:, :kv_width]
        key_buf[k * rows:(k + 1) * rows, :] = jnp.dot(
            piece_lat, kup_ref[...], preferred_element_type=F32
        ).astype(BF)
        val_buf[k * rows:(k + 1) * rows, :] = jnp.dot(
            piece_lat, vup_ref[...], preferred_element_type=F32
        ).astype(BF)

    for load in loads[2:10]:
        load.wait()
    make_kv(0)
    query_rot = turn(
        turn_ref[...].astype(F32),
        jnp.concatenate([cosine] * (turn_ref.shape[1] // 128), axis=1),
        jnp.concatenate([sine] * (turn_ref.shape[1] // 128), axis=1),
    ).astype(BF)

    def pass_latent(slot, quarter):
        piece = kv_buf.at[slot, quarter]
        send(piece, piece, f_ssem.at[0], f_rsem.at[slot], (s, other))

    def take_latent(slot):
        piece = kv_buf.at[slot, t]
        arrived(piece, l_rsem.at[slot])
        send(piece, piece, c_ssem.at[0], c_rsem.at[slot], along_x)
        pass_latent(slot, t)

    take_latent(1)
    for by in (6, 4, 2):
        send_latent(1, by)
    loads[10].wait()
    send_relays(2)
    order = (2, 4, 6, 3, 5, 7)
    for slot in order:
        take_latent(slot)
    send_by_place(first)
    def take_block(slot):
        arrived(kv_buf.at[slot, pl.ds(0, tp // 2)], f_rsem.at[slot])
        make_kv(slot)

    order = (1,) + order
    for i, slot in enumerate(order):
        arrived(kv_buf.at[slot, along_x[1]], c_rsem.at[slot])
        pass_latent(slot, along_x[1])
        if i > 1:
            take_block(order[i - 2])
    for slot in order[-2:]:
        take_block(slot)

    scale = (NOPE + ROPE) ** (-0.5) * math.log2(math.e)
    all_rot = kv_buf[...].reshape(sp * rows, kv_buf.shape[3])[:, kv_width:]
    lane = lax.broadcasted_iota(jnp.int32, (rows, 128), 1)
    for pair in range(query_ref.shape[1] // 128):
        span = slice(pair * 128, (pair + 1) * 128)
        keys = jnp.concatenate([key_buf[:, span], all_rot], axis=1)
        vals = val_buf[:, span]
        results = []
        for inner in range(2):
            head = pair * 2 + inner
            tile = head * ROPE // 128
            group = head % (128 // ROPE)
            q_plain = jnp.where(lane // NOPE == inner, query_ref[:, span], jnp.zeros((), BF))
            q_turn = jnp.where(
                lane // ROPE == group, query_rot[:, tile * 128:(tile + 1) * 128], jnp.zeros((), BF)
            )
            score = lax.dot_general(
                jnp.concatenate([q_plain, q_turn], axis=1), keys, BY_LAST, preferred_element_type=F32
            )
            top = jnp.max(score, axis=-1, keepdims=True)
            expo = jnp.exp2((score - top) * scale)
            total = jnp.sum(expo, axis=-1, keepdims=True)
            results.append(jnp.dot(expo.astype(BF), vals, preferred_element_type=F32) / total)
        att_buf[:, span] = jnp.where(lane < V, results[0], results[1]).astype(BF)

    relayed(0)
    send_by_place(between)
    span_of = [slice(c * width // 2, (c + 1) * width // 2) for c in range(2)]
    for c, span in enumerate(span_of):
        mix = jnp.dot(att_buf[...], ow_ref[:, span], preferred_element_type=F32)
        mix_buf[:, span] = mix
        for dest in range(tp):
            pair_buf[dest % 2, c, dest // 2] = mix[dest * part:(dest + 1) * part].astype(BF)
        send(pair_buf.at[1 - core, c], paird_buf.at[c], m_ssem.at[0], m_rsem.at[c], (s, other))
    cross_rows = pl.ds(pl.multiple_of(((1 - x) * 2 + core) * part, part), part)
    for c, span in enumerate(span_of):
        arrived(paird_buf.at[c], m_rsem.at[c])
        cross_buf[c] = (mix_buf[cross_rows, span] + paird_buf[c, 1 - x].astype(F32)).astype(BF)
        send(cross_buf.at[c], crossr_buf.at[c], m_ssem.at[1], m_rsem.at[2 + c], along_x)
    mids = [
        resid_ref[:, span].astype(F32) + mix_buf[own_rows, span] + paird_buf[c, x].astype(F32)
        for c, span in enumerate(span_of)
    ]
    for c in range(2):
        arrived(crossr_buf.at[c], m_rsem.at[2 + c])
        mids[c] = mids[c] + crossr_buf[c].astype(F32)
    mid = jnp.concatenate(mids, axis=1)
    mid_buf[...] = mid
    normed = mid * lax.rsqrt(jnp.mean(mid * mid, axis=-1, keepdims=True) + 1e-06) * mgain_ref[...]
    n_buf[0] = normed.astype(BF)

    a_x = 1 - core
    pick = lambda first_x, i: first_x * along_x[i] + (1 - first_x) * along_y[i]
    steps = (
        (8, (pick(a_x, 0), pick(a_x, 1))),
        (4, (pick(core, 0), pick(core, 1))),
        (2, (ring(2), t)),
        (1, (ring(4), t)),
    )

    def spread(slot):
        for by, dev in reversed(steps):
            if by > slot:
                to = slot + by
                send(n_buf.at[slot], n_buf.at[to], a_ssem.at[0], a_rsem.at[min(to, sp)], dev)

    spread(0)
    relayed(1)
    send_by_place(second)
    arrived(n_buf.at[1], a_rsem.at[1])
    spread(1)
    send_by_place(third)
    relayed(2)
    send_weights(fourth)
    for slot in (2, 3):
        arrived(n_buf.at[slot], a_rsem.at[slot])
        spread(slot)
    for slot in (4, 5, 6, 7):
        arrived(n_buf.at[slot], a_rsem.at[slot])
        spread(slot)
    pass_weights(0, 0)
    pass_weights(1, 0)
    pass_weights(0, 1)
    pass_weights(1, 1)
    group = n_buf.shape[0] // 2

    def hidden_of(side):
        for g in range(2):
            block = n_buf[g * group:(g + 1) * group].reshape(group * part, width)
            gate = lax.dot_general(block, w_buf[0, side], BY_LAST, preferred_element_type=F32)
            up = lax.dot_general(block, w_buf[1, side], BY_LAST, preferred_element_type=F32)
            hidden = (gate / (1.0 + jnp.exp(-gate)) * up).astype(BF)
            for k in range(group):
                slot = k % 2 * 8 + g * 4 + k // 2 % 2 * 2 + k // 4
                h_buf[side, slot * part:(slot + 1) * part, :] = hidden[k * part:(k + 1) * part]

    arrived(n_buf.at[pl.ds(group, group)], a_rsem.at[sp])
    hidden_of(core)
    passed_weights(0)
    passed_weights(1)
    hidden_of(1 - core)

    last = (3,)
    to_first, to_second, to_low, to_high = (dev for by, dev in steps)
    messages = {
        14: (2, to_first),
        12: (2, to_first),
        10: (2, to_low),
        9: (1, to_second),
        8: (1, to_high),
        6: (2, to_first),
        4: (2, to_first),
        2: (2, to_low),
        1: (1, to_second),
    }
    index_of = {slot: i for i, slot in enumerate((*messages, 3))}

    def over(q):
        return (ring(q + 1 - core), t + core * (along_x[1] - t))

    direct = {**messages, 3: (1, over(2)), 2: (1, to_low), 9: (1, over(4))}

    def message(q, slot):
        return direct[slot] if q in last else messages[slot]

    def sums(q, slot):
        count, dev = message(q, slot)
        some = pl.ds(slot, count)
        send(acc_buf.at[q, some], r_buf.at[q, some], s_ssem.at[0], s_rsem.at[q, index_of[slot]], dev)

    def project(q):
        h, columns = q // 2, slice(q % 2 * quarter, (q % 2 + 1) * quarter)
        for g in (1, 0):
            span = slice(g * group * part, (g + 1) * group * part)
            down = jnp.dot(
                h_buf[0, span], wd_buf[h, 0, :, columns], preferred_element_type=F32
            ) + jnp.dot(h_buf[1, span], wd_buf[h, 1, :, columns], preferred_element_type=F32)
            acc_buf[q, g * group:(g + 1) * group] = down.astype(BF).reshape(group, part, quarter)
            sums(q, g * group + 6)
            sums(q, g * group + 4)

    def landed(q, slot):
        count = message(q, slot)[0]
        arrived(r_buf.at[q, pl.ds(slot, count)], s_rsem.at[q, index_of[slot]])
        return r_buf[q, slot:slot + count].astype(F32)

    def join(q, to, *slots):
        count = message(q, slots[0])[0]
        value = acc_buf[q, to:to + count].astype(F32)
        for slot in slots:
            value = value + landed(q, slot)
        acc_buf[q, to:to + count] = value.astype(BF)

    def to_10(q):
        join(q, 10, 14)
        sums(q, 10)

    def to_2(q):
        join(q, 2, 6)
        if q in last:
            sums(q, 3)
        sums(q, 2)

    def to_9(q):
        join(q, 8, 12, 10)
        sums(q, 9)
        if q in last:
            sums(q, 8)

    def to_8(q):
        if q not in last:
            join(q, 8, 9)
            sums(q, 8)

    def to_1(q):
        join(q, 0, *((4,) if q in last else (4, 2)))
        sums(q, 1)

    def finish(q):
        value = acc_buf[q, 0].astype(F32)
        for slot in (2, 3, 9, 1, 8) if q in last else (1, 8):
            value = value + landed(q, slot)[0]
        h, c = q // 2, q % 2
        for k in range(sp // 2):
            z = (1 + k // 2) if c == 0 else 3 * (k // 2)
            start = (2 * z + k % 2) * cols + h * lanes
            span = slice(start, start + lanes)
            out_ref[:, span] = (
                mid_buf[:, span] + 0.5 * value[:, k * lanes:(k + 1) * lanes]
            ).astype(BF)

    pass_down(0)
    passed_down(0)
    project(0)
    pass_down(1)
    passed_down(1)
    project(1)
    to_10(0)
    to_2(0)
    pass_down(2)
    passed_down(2)
    project(2)
    to_10(1)
    to_9(0)
    to_2(1)
    pass_down(3)
    passed_down(3)
    project(3)
    to_9(1)
    to_10(2)
    to_2(2)
    to_8(0)
    to_10(3)
    to_8(1)
    to_9(2)
    to_2(3)
    to_1(0)
    to_1(1)
    to_8(2)
    to_9(3)
    to_1(2)
    to_1(3)
    finish(0)
    finish(1)
    finish(2)
    finish(3)

    rest = pl.ds(1, sp - 1)
    sent(r_buf.at[:, pl.ds(1, 2 * sp - 1)], s_ssem.at[0])
    sent(n_buf.at[pl.ds(1, 2 * sp - 1)], a_ssem.at[0])
    sent(paird_buf, m_ssem.at[0])
    sent(crossr_buf, m_ssem.at[1])
    sent(kv_buf.at[rest, 0], l_ssem.at[0])
    sent(kv_buf.at[rest, 0], c_ssem.at[0])
    sent(kv_buf.at[rest, pl.ds(0, tp // 2)], f_ssem.at[0])
    sent(relay_buf, y_ssem.at[0])
    sent(w_buf.at[:, 0, :, :(sp - 1) * cols], w_ssem.at[0])
    sent(wd_buf.at[:, 0, :, :(sp - 1) * lanes], w_ssem.at[1])
    sent(w_buf.at[:, 0], x_ssem.at[0])
    sent(wd_buf.at[:, 0], x_ssem.at[1])


def fused_layer(
    resid_in,
    query_plain,
    query_turn,
    latent_raw,
    shared_key,
    latent_gain,
    key_up,
    value_up,
    out_weight,
    mixer_gain,
    gate_weight,
    up_weight,
    down_weight,
):
    sp = lax.axis_size("sp")
    tp = lax.axis_size("tp")
    rows, width = resid_in.shape
    part = rows // tp
    hid = down_weight.shape[0] // sp
    cols = down_weight.shape[1]
    kv = latent_raw.shape[1]
    heads_width = query_plain.shape[1]
    inverse = 10000.0 ** (-jnp.arange(0, ROPE, 2, dtype=F32) / ROPE)
    inverse_lanes = jnp.tile(inverse, 128 * 2 // ROPE)[None, :]
    chips = sp * tp // 2
    dma = pltpu.SemaphoreType.DMA
    vmem = lambda *shape: pltpu.VMEM(shape, BF)
    near = pl.BlockSpec(memory_space=pltpu.VMEM)
    far = pl.BlockSpec(memory_space=pl.ANY)
    return pl.pallas_call(
        functools.partial(layer_kernel, (sp, tp)),
        out_shape=pltpu.VMEM((part, width), BF),
        in_specs=[near] * 5 + [far] * 9,
        out_specs=near,
        scratch_shapes=[
            vmem(*query_plain.shape),
            vmem(*query_turn.shape),
            vmem(*key_up.shape),
            vmem(*value_up.shape),
            vmem(*out_weight.shape),
            vmem(part, width),
            vmem(2, *gate_weight.shape),
            vmem(3, sp, hid, cols),
            vmem(3, sp // 2 - 1, hid, cols),
            vmem(sp, tp, part, kv + 128),
            vmem(sp * rows, heads_width),
            vmem(sp * rows, heads_width),
            vmem(rows, heads_width),
            pltpu.VMEM((rows, width), F32),
            vmem(2, 2, tp // 2, part, width // 2),
            vmem(2, tp // 2, part, width // 2),
            vmem(2, part, width // 2),
            vmem(2, part, width // 2),
            pltpu.VMEM((part, width), F32),
            vmem(2, 2, hid, width),
            vmem(2, 2, hid, width // 2),
            vmem(chips, part, width),
            vmem(2, chips * part, hid),
            vmem(4, chips, part, width // 4),
            vmem(4, chips, part, width // 4),
            dma((11,)),
            dma((1,)),
            dma((sp,)),
            dma((1,)),
            dma((sp,)),
            dma((1,)),
            dma((sp,)),
            dma((2,)),
            dma((4,)),
            dma((2,)),
            dma((4, 2)),
            dma((1,)),
            dma((3,)),
            dma((2,)),
            dma((6,)),
            dma((1,)),
            dma((sp + 1,)),
            dma((1,)),
            dma((4, sp + 2)),
        ],
        compiler_params=pltpu.CompilerParams(
            collective_id=0, has_side_effects=True, vmem_limit_bytes=60 * 1024 * 1024
        ),
    )(
        latent_raw,
        shared_key.T,
        inverse_lanes,
        latent_gain[None, :],
        mixer_gain[None, :],
        query_plain,
        query_turn,
        key_up,
        value_up,
        out_weight,
        resid_in,
        gate_weight,
        up_weight,
        down_weight.reshape(sp, hid, cols),
    )


def per_device(*arrays):
    resid_in, query_plain, query_turn, latent_raw = arrays[:4]
    down_weight = arrays[-1]
    sp = lax.axis_size("sp")
    tp = lax.axis_size("tp")
    rows = resid_in.shape[0]
    fits = (
        sp // 4 == 2
        and tp // 2 == 2
        and rows % (32 * tp) == 0
        and down_weight.shape[0] % (16 * sp) == 0
        and down_weight.shape[1] % 128 == 0
        and latent_raw.shape[1] % 128 == 0
        and query_plain.shape[1] % 128 == 0
        and query_turn.shape[1] % 128 == 0
        and rows * sp <= 1024
        and sp * tp <= 32
    )
    if fits:
        return fused_layer(*arrays)
    return plain_layer(*arrays)


def solution(mesh):
    return jax.shard_map(
        per_device,
        mesh=mesh,
        in_specs=(
            P("sp", None),
            P("sp", "tp"),
            P("sp", "tp"),
            P("sp", None),
            P("sp", None),
            P(),
            P(None, "tp"),
            P(None, "tp"),
            P("tp", None),
            P(),
            P("sp", "tp"),
            P("sp", "tp"),
            P("tp", "sp"),
        ),
        out_specs=P(("sp", "tp"), None),
        check_vma=False,
    )
```
